512 devices in a mesh: grp: 2 (over y), kv: 32 (over z), tp: 8 (over x, core).
Axes of the slice: x: 4, y: 2, z: 32, core: 2. Of those that a mesh axis runs over, the one named last changes fastest.
The devices are a block of a 4x8x32 slice.
Arguments:
- tokens: bfloat16 [1536, 4096], P('grp', 'kv'), parts along dimension 0, may hold values from -40 to 40
- norm_gain: bfloat16 [4096], P('kv'), may hold values from 0.099609375 to 1.8984375
- w_query: bfloat16 [4096, 2048], P('kv', 'tp'), may hold values from -0.09375 to 0.09375
- w_key: bfloat16 [4096, 2048], P('kv', 'tp'), may hold values from -0.09375 to 0.09375
- w_value: bfloat16 [4096, 2048], P('kv', 'tp'), may hold values from -0.09375 to 0.09375
- w_gate: bfloat16 [4096, 2048], P('kv', 'tp'), may hold values from -0.09375 to 0.09375
- w_beta: bfloat16 [4096, 16], replicated, may hold values from -0.09375 to 0.09375
- w_decay: bfloat16 [4096, 16], replicated, may hold values from -0.09375 to 0.09375
- decay_rate: float32 [16], P('tp'), may hold values from 0.05 to 1.5
- out_gain: bfloat16 [128], replicated, may hold values from 0.099609375 to 1.8984375
- w_out: bfloat16 [2048, 4096], P('tp', 'kv'), may hold values from -0.125 to 0.125
- state: float32 [512, 16, 128, 128], P(('grp', 'kv'), 'tp'), parts along dimension 0, may hold values from -6 to 6
- prev_keys: bfloat16 [512, 3, 16, 128], P(('grp', 'kv'), None, 'tp'), parts along dimension 0, may hold values from -6 to 6
- prev_values: bfloat16 [512, 3, 16, 128], P(('grp', 'kv'), None, 'tp'), parts along dimension 0, may hold values from -6 to 6
- prev_beta: float32 [512, 3, 16], P(('grp', 'kv'), None, 'tp'), parts along dimension 0, may hold values from 0.2 to 1
- prev_logdecay: float32 [512, 3, 16], P(('grp', 'kv'), None, 'tp'), parts along dimension 0, may hold values from -1.5 to -0.05
- accepted: int32 [512], P(('grp', 'kv')), parts along dimension 0, may hold values from 0 to 3
Outputs:
- mixed: bfloat16 [1536, 4096], P('grp', 'kv'), parts along dimension 0
- new_state: float32 [512, 16, 128, 128], P(('grp', 'kv'), 'tp'), parts along dimension 0
The draws below stay inside these ranges and needn't reach their ends.
There are 2 independent parts, one for each index of `grp`. The reference program is written for one: setup_inputs(seed, part) draws one part's arguments, and reference() takes and returns one part's arrays. A program takes and returns all parts, laid end to end along the dimension named above; an argument that names none is the same for every part. Nothing has to cross between parts.
All inputs are finite; a program needn't handle non-finite values.
Results may differ from the reference program's by a relative error of at most 0.0071.
Values may be sent and summed in bfloat16 or wider, within the bound.
No kernel may reach another device: no remote copies, remote signals or barrier semaphores. Data moves between devices by JAX's collectives and lax.ppermute only.
A program may use at most 64 MiB of HBM per device.

```python
import math
import jax
import jax.numpy as jnp
from jax import lax

D = 4096
H = 16
DK = 128
P_SIZE = 3
SEQS = 256
TOKENS = 768


def draw_tokens(key, part):
    first = jax.random.fold_in(key, 0)
    column_scale = jnp.exp(jnp.log(3.0) * jnp.arange(D, dtype=jnp.float32) / D)[None, :]
    base = jnp.clip(jax.random.normal(first, (TOKENS, D), jnp.float32), -4.0, 4.0)
    values = base * column_scale
    return jnp.clip(values, -40.0, 40.0).astype(jnp.bfloat16)


def with_ends(drawn, own_key, least, high):
    longest = drawn.shape.index(max(drawn.shape))
    spots = []
    for shift in (0, 1):
        where = [jax.random.randint(jax.random.fold_in(own_key, axis), (), 0, length) for axis, length in enumerate(drawn.shape)]
        where[longest] = (where[longest] + shift) % drawn.shape[longest]
        spots.append(tuple(where))
    return drawn.at[spots[0]].set(least).at[spots[1]].set(high)


def levels(key, shape, cuts, smallest, high):
    def one(axis_at, blocks):
        heights = jax.random.uniform(jax.random.fold_in(jax.random.fold_in(key, 6), axis_at), (blocks,), jnp.float32, smallest / len(cuts), high / len(cuts))
        return jnp.repeat(jnp.exp(heights), shape[axis_at] // blocks).reshape((-1,) + (1,) * (len(shape) - axis_at - 1))

    level = one(*cuts[0])
    for cut in cuts[1:]:
        level = level * one(*cut)
    return level


def gaussian(stream_key, shape, deviation, limit, pieces=(), kind=jnp.bfloat16):
    level = levels(stream_key, shape, pieces, -0.22, 0.18) if pieces else 1.0
    array = jax.random.normal(stream_key, shape, jnp.float32) * deviation * level
    return jnp.minimum(jnp.maximum(array, -limit), limit).astype(kind)


def setup_inputs(seed: int = 0, part: int = 0) -> dict:
    arg_keys = jax.random.split(jax.random.key(seed), 18)
    part_splits = jax.random.split(jax.random.fold_in(arg_keys[17], part), 18)
    return {
        "tokens": draw_tokens(jax.random.fold_in(jax.random.fold_in(arg_keys[17], part), 71), part),
        "norm_gain": jnp.clip(1.0 + 0.18 * jax.random.normal(arg_keys[1], (D,), jnp.float32), 0.099609375, 1.8984375).astype(jnp.bfloat16),
        "w_query": gaussian(arg_keys[2], (D, H * DK), D ** -0.5, 0.09375, ((0, 32), (1, 8))),
        "w_key": gaussian(arg_keys[3], (D, H * DK), D ** -0.5, 0.09375, ((0, 32), (1, 8))),
        "w_value": gaussian(arg_keys[4], (D, H * DK), D ** -0.5, 0.09375, ((0, 32), (1, 8))),
        "w_gate": gaussian(arg_keys[5], (D, H * DK), D ** -0.5, 0.09375, ((0, 32), (1, 8))),
        "w_beta": gaussian(arg_keys[6], (D, H), D ** -0.5, 0.09375),
        "w_decay": gaussian(arg_keys[7], (D, H), D ** -0.5, 0.09375),
        "decay_rate": jnp.clip(jnp.exp(math.log(1.5) - 3.4011974 * jax.random.uniform(arg_keys[8], (H,), jnp.float32) ** levels(arg_keys[8], (H,), ((0, 8),), -0.2, 0.2)), 0.05, 1.5),
        "out_gain": jnp.clip(1.0 + 0.18 * jax.random.normal(arg_keys[9], (DK,), jnp.float32), 0.099609375, 1.8984375).astype(jnp.bfloat16),
        "w_out": gaussian(arg_keys[10], (H * DK, D), (H * DK) ** -0.5, 0.125, ((0, 8), (1, 32))),
        "state": gaussian(part_splits[11], (SEQS, H, DK, DK), 1.0, 6.0, ((0, 32), (1, 8)), jnp.float32),
        "prev_keys": gaussian(part_splits[12], (SEQS, P_SIZE, H, DK), 1.0, 6.0, ((0, 32), (2, 8))),
        "prev_values": gaussian(part_splits[13], (SEQS, P_SIZE, H, DK), 1.0, 6.0, ((0, 32), (2, 8))),
        "prev_beta": jnp.clip(0.2 + 0.8 * jax.random.uniform(part_splits[14], (SEQS, P_SIZE, H), jnp.float32) ** levels(part_splits[14], (SEQS, P_SIZE, H), ((0, 32), (2, 8)), -0.2, 0.2), 0.2, 1.0),
        "prev_logdecay": jnp.clip(-1.5 + 1.45 * jax.random.uniform(part_splits[15], (SEQS, P_SIZE, H), jnp.float32) ** levels(part_splits[15], (SEQS, P_SIZE, H), ((0, 32), (2, 8)), -0.2, 0.2), -1.5, -0.05),
        "accepted": with_ends(jax.random.randint(part_splits[16], (SEQS,), 0, P_SIZE + 1), jax.random.fold_in(part_splits[16], 1), 0, P_SIZE).astype(jnp.int32),
    }


EPS = 1e-06
HIGHEST = lax.Precision.HIGHEST

def unit_rows(vectors):
    return vectors * lax.rsqrt(lax.optimization_barrier(jnp.sum(vectors * vectors, axis=-1, keepdims=True)) + EPS)

def replay(carry_state, prev_keys, prev_values, prev_beta, prev_logdecay, accepted):
    span_size = prev_keys.shape[1]
    unit_keys = unit_rows(prev_keys.astype(jnp.float32))
    value_rows = prev_values.astype(jnp.float32)
    for position in range(span_size):
        active = (accepted > position)[:, None]
        factor = jnp.exp(jnp.where(active, prev_logdecay[:, position], jnp.float32(0.0)))
        strength = jnp.where(active, prev_beta[:, position], jnp.float32(0.0))
        decayed = factor[:, :, None, None] * carry_state
        current_key = unit_keys[:, position]
        predicted = jnp.einsum('bhde,bhd->bhe', decayed, current_key, precision=HIGHEST)
        update = strength[:, :, None] * (value_rows[:, position] - predicted)
        carry_state = decayed + current_key[:, :, :, None] * update[:, :, None, :]
    return carry_state

def propose(carry_state, queries, key_rows, value_rows, beta_rows, log_decay):
    span_size = queries.shape[1]
    head_queries = jnp.moveaxis(queries, 1, 2)
    head_keys = jnp.moveaxis(key_rows, 1, 2)
    head_values = jnp.moveaxis(value_rows, 1, 2)
    head_beta = jnp.moveaxis(beta_rows, 1, 2)
    cumulative = jnp.cumsum(jnp.moveaxis(log_decay, 1, 2), axis=-1)
    order = jnp.arange(span_size)
    inclusive = order[:, None] >= order[None, :]
    strict = order[:, None] > order[None, :]
    spread = cumulative[..., :, None] - cumulative[..., None, :]
    within = jnp.where(inclusive, jnp.exp(jnp.where(inclusive, spread, jnp.float32(0.0))), jnp.float32(0.0))
    weighted_keys = head_keys * head_beta[..., None]
    lower = jnp.where(strict, jnp.einsum('bhid,bhjd->bhij', weighted_keys, head_keys, precision=HIGHEST) * within, jnp.float32(0.0))
    right_side = jnp.concatenate([head_values * head_beta[..., None], weighted_keys * jnp.exp(cumulative)[..., None]], axis=-1)
    solved = []
    for row in range(span_size):
        current = right_side[:, :, row]
        for column in range(row):
            current = current - lower[:, :, row, column][..., None] * solved[column]
        solved.append(current)
    solved = jnp.stack(solved, axis=2)
    depth = head_values.shape[-1]
    corrections = solved[..., :depth] - jnp.einsum('bhcd,bhde->bhce', solved[..., depth:], carry_state, precision=HIGHEST)
    scores = jnp.einsum('bhid,bhjd->bhij', head_queries, head_keys, precision=HIGHEST) * within
    outputs = jnp.einsum('bhcd,bhde->bhce', head_queries * jnp.exp(cumulative)[..., None], carry_state, precision=HIGHEST)
    outputs = outputs + jnp.einsum('bhij,bhje->bhie', scores, corrections, precision=HIGHEST)
    return jnp.moveaxis(outputs, 2, 1)

def finish(heads_out, gate_rows, out_gain):
    scale = lax.rsqrt(lax.optimization_barrier(jnp.mean(heads_out * heads_out, axis=-1, keepdims=True)) + EPS)
    return (heads_out * scale * out_gain.astype(jnp.float32) * jax.nn.silu(gate_rows)).astype(jnp.bfloat16)

def reference(tokens, norm_gain, w_query, w_key, w_value, w_gate, w_beta, w_decay, decay_rate, out_gain, w_out, state, prev_keys, prev_values, prev_beta, prev_logdecay, accepted):
    widened = tokens.astype(jnp.float32)
    inverse = lax.rsqrt(lax.optimization_barrier(jnp.sum(widened * widened, axis=1)) / D + EPS)[:, None]
    scaled = (widened * norm_gain.astype(jnp.float32)).astype(jnp.bfloat16)

    def project(weight):
        return jnp.dot(scaled, weight, preferred_element_type=jnp.float32) * inverse
    shape_heads = (SEQS, P_SIZE, H, DK)
    queries = unit_rows(project(w_query).reshape(shape_heads)) * DK ** (-0.5)
    key_rows = unit_rows(project(w_key).reshape(shape_heads))
    value_rows = project(w_value).reshape(shape_heads)
    gate_rows = project(w_gate).reshape(shape_heads)
    beta_rows = jax.nn.sigmoid(project(w_beta).reshape(SEQS, P_SIZE, H))
    log_decay = -decay_rate * jax.nn.softplus(project(w_decay).reshape(SEQS, P_SIZE, H))
    carried = replay(state, prev_keys, prev_values, prev_beta, prev_logdecay, accepted)
    heads_out = propose(carried, queries, key_rows, value_rows, beta_rows, log_decay)
    hidden = finish(heads_out, gate_rows, out_gain).reshape(TOKENS, H * DK)
    summed = jnp.dot(hidden, w_out, preferred_element_type=jnp.float32)
    return (summed.astype(jnp.bfloat16), carried)
```

```python
import jax
import jax.numpy as jnp
from jax import lax
from jax.experimental import pallas as pl
from jax.experimental.pallas import tpu as pltpu
from jax.sharding import PartitionSpec as P

EPS = 1e-06
NEAR = 4
NEAR_OUT = 8
LANES = 128
HALF = LANES // 2
F32 = jnp.float32
BF16 = jnp.bfloat16


def shift(table, axis_size, by):
    return lax.ppermute(table, "kv", [(i, (i + by) % axis_size) for i in range(axis_size)])


def replay_body(keys_ref, values_ref, beta_ref, logdecay_ref, accepted_ref, state_ref, out_ref):
    seq = pl.program_id(0)
    heads_here, depth = state_ref.shape[1], state_ref.shape[2]
    span_size = keys_ref.shape[1] // heads_here
    for head in range(heads_here):
        carry = state_ref[0, head]
        for position in range(span_size):
            row = position * heads_here + head
            active = accepted_ref[seq] > position
            spot = seq * span_size * heads_here + row
            logdecay = jnp.where(active, logdecay_ref[spot], F32(0.0))
            strength = jnp.where(active, beta_ref[spot], F32(0.0))
            factor = jnp.exp(jnp.full((1, depth), logdecay, F32))
            key = keys_ref[0, row : row + 1, :]
            key = key * lax.rsqrt(jnp.sum(key * key, axis=-1, keepdims=True) + EPS)
            key_columns = jnp.transpose(jnp.broadcast_to(key, (depth, depth)))
            carry = factor * carry
            predicted = jnp.sum(key_columns * carry, axis=0, keepdims=True)
            update = strength * (values_ref[0, row : row + 1, :] - predicted)
            carry = carry + key_columns * update
        out_ref[0, head] = carry


def replay(state, prev_keys, prev_values, prev_beta, prev_logdecay, accepted):
    seq_count, heads_here, depth, _ = state.shape
    rows = prev_keys.shape[1] * heads_here
    keys = prev_keys.astype(F32).reshape(seq_count, rows, depth)
    values = prev_values.astype(F32).reshape(seq_count, rows, depth)
    row_spec = pl.BlockSpec((1, rows, depth), lambda b: (b, 0, 0))
    state_spec = pl.BlockSpec((1, heads_here, depth, depth), lambda b: (b, 0, 0, 0))
    smem = pl.BlockSpec(memory_space=pltpu.SMEM)
    return pl.pallas_call(
        replay_body,
        grid=(seq_count,),
        in_specs=[row_spec, row_spec, smem, smem, smem, state_spec],
        out_specs=state_spec,
        out_shape=jax.ShapeDtypeStruct(state.shape, F32),
        name="replay",
    )(keys, values, prev_beta.reshape(-1), prev_logdecay.reshape(-1), accepted, state)


def class_rows(wide_ref, which, own_rows):
    members = wide_ref.shape[0] // (NEAR * own_rows)
    starts = [pl.multiple_of((member * NEAR + which) * own_rows, 8) for member in range(members)]
    return jnp.concatenate([wide_ref[pl.ds(start, own_rows), :] for start in starts], axis=0)


def side_by_side(rows):
    half = rows.shape[0] // 2
    return jnp.concatenate([rows[:half], rows[half:]], axis=1).astype(BF16)


def pack_body(own_rows, place_ref, tokens_ref, gain_ref, wq_ref, wk_ref, wv_ref, wg_ref, next_ref, previous_ref, wide_ref):
    columns = gain_ref.shape[1]
    wide_ref[...] = tokens_ref[...].astype(F32)
    gain = jnp.concatenate([gain_ref[...]] * (wq_ref.shape[1] // columns), axis=1)
    gain = jnp.broadcast_to(gain, (16, wq_ref.shape[1]))
    for out_ref in (next_ref, previous_ref):
        for j, weight_ref in enumerate((wq_ref, wk_ref, wv_ref, wg_ref)):
            out_ref[j * columns : (j + 1) * columns, :] = weight_ref[...]
        out_ref[4 * columns : 4 * columns + 16, :] = gain
    rows_at = 4 * columns + 16
    shard_kv = place_ref[0]
    packed = side_by_side(class_rows(wide_ref, (shard_kv + 1) % NEAR, own_rows))
    half = packed.shape[0]
    next_ref[rows_at:, :] = packed
    previous_ref[rows_at : rows_at + half, :] = side_by_side(class_rows(wide_ref, (shard_kv + NEAR - 2) % NEAR, own_rows))
    previous_ref[rows_at + half :, :] = side_by_side(class_rows(wide_ref, (shard_kv + NEAR - 1) % NEAR, own_rows))


def pack(place, tokens, gain, weights, own_rows):
    rows, columns = tokens.shape
    wide = weights[0].shape[1]
    held = 4 * columns + 16
    half = rows // NEAR // 2
    smem = pl.BlockSpec(memory_space=pltpu.SMEM)
    vmem = pl.BlockSpec(memory_space=pltpu.VMEM)

    def body(*refs):
        pack_body(own_rows, *refs)

    return pl.pallas_call(
        body,
        in_specs=[smem] + [vmem] * 6,
        out_specs=[vmem, vmem],
        out_shape=[
            jax.ShapeDtypeStruct((held + half, wide), BF16),
            jax.ShapeDtypeStruct((held + 2 * half, wide), BF16),
        ],
        scratch_shapes=[pltpu.VMEM((rows, columns), F32)],
        name="pack",
    )(place, tokens, gain, *weights)


def split(values, wide):
    small = values[:, wide:]
    lane = lax.broadcasted_iota(jnp.int32, small.shape, 1)
    coarse = small.astype(BF16).astype(F32)
    rest = pltpu.roll(small - coarse, HALF, 1)
    return values[:, :wide].astype(BF16), jnp.where(lane < HALF, coarse, rest).astype(BF16)


def joined(terms, wide):
    small = terms[:, wide:].astype(F32)
    lane = lax.broadcasted_iota(jnp.int32, small.shape, 1)
    small = jnp.where(lane < HALF, small + pltpu.roll(small, HALF, 1), F32(0.0))
    return terms[:, :wide].astype(F32), small


def project_body(
    own_rows,
    place_ref,
    tokens_ref,
    gain_ref,
    wq_ref,
    wk_ref,
    wv_ref,
    wg_ref,
    s0,
    s1,
    s2,
    s3,
    before_ref,
    after_ref,
    far_ref,
    up_ref,
    down_ref,
    across_ref,
    kept_ref,
    wide_ref,
    sums_ref,
):
    columns = gain_ref.shape[1]
    wide = wq_ref.shape[1]
    half = tokens_ref.shape[0] // NEAR // 2
    members = 2 * half // own_rows
    gain_at = 4 * columns
    shard_kv = place_ref[0]
    wide_ref[...] = tokens_ref[...].astype(F32)

    def taken(pay_ref, rows_at):
        weights = [pay_ref[j * columns : (j + 1) * columns, :] for j in range(4)]
        gain = pay_ref[gain_at : gain_at + 16, :columns].astype(F32)[:1]
        both = pay_ref[rows_at : rows_at + half, :].astype(F32)
        return jnp.concatenate([both[:, :columns], both[:, columns:]], axis=0), gain, weights

    own = (
        class_rows(wide_ref, shard_kv % NEAR, own_rows),
        gain_ref[...].astype(F32),
        [wq_ref[...], wk_ref[...], wv_ref[...], wg_ref[...]],
    )
    first = gain_at + 16
    parts = [(taken(before_ref, first), s0), (own, s1), (taken(after_ref, first + half), s2), (taken(far_ref, first), s3)]
    sums = [None] * 4
    small = None
    squares = None
    for (widened, gain, weights), small_ref in parts:
        term = jnp.sum(widened * widened, axis=1, keepdims=True)
        squares = term if squares is None else squares + term
        scaled = (widened * gain).astype(BF16)
        for j in range(4):
            term = jnp.dot(scaled, weights[j], preferred_element_type=F32)
            sums[j] = term if sums[j] is None else sums[j] + term
        term = jnp.dot(scaled, small_ref[...], preferred_element_type=F32)
        small = term if small is None else small + term
    lane = lax.broadcasted_iota(jnp.int32, small.shape, 1)
    small = jnp.where(lane == HALF - 1, squares, small)
    for j in range(4):
        sums_ref[:, j * wide : (j + 1) * wide] = sums[j]
    sums_ref[:, 4 * wide :] = small

    def block(ahead):
        start = ((shard_kv // NEAR + members + ahead) % members) * own_rows
        return sums_ref[pl.ds(pl.multiple_of(start, 8), own_rows), :]

    for out_ref, at, ahead in (
        (up_ref, 0, 1),
        (up_ref, 1, 3),
        (down_ref, 0, -1),
        (down_ref, 1, -3),
        (across_ref, 0, 4),
    ):
        big, little = split(block(ahead), 4 * wide)
        out_ref[at, :, : 4 * wide] = big
        out_ref[at, :, 4 * wide :] = little
    for at, ahead in enumerate((0, 2, -2)):
        kept_ref[at] = block(ahead)


def project(place, tokens, gain, weights, small_weights, before, after, far, own_rows):
    rows, columns = tokens.shape
    wide = weights[0].shape[1]
    across = 4 * wide + LANES
    whole = lambda a: pl.BlockSpec(a.shape, lambda i, w: (0,) * a.ndim)
    small_specs = [pl.BlockSpec((columns, LANES), lambda i, w, n=n: (w[1 + n], 0)) for n in range(4)]
    operands = [tokens, gain, *weights]
    shapes = [
        jax.ShapeDtypeStruct((2, own_rows, across), BF16),
        jax.ShapeDtypeStruct((2, own_rows, across), BF16),
        jax.ShapeDtypeStruct((1, own_rows, across), BF16),
        jax.ShapeDtypeStruct((3, own_rows, across), F32),
    ]

    def body(*refs):
        project_body(own_rows, *refs)

    return pl.pallas_call(
        body,
        grid_spec=pltpu.PrefetchScalarGridSpec(
            num_scalar_prefetch=1,
            grid=(1,),
            in_specs=[whole(a) for a in operands] + small_specs + [whole(a) for a in (before, after, far)],
            out_specs=[whole(a) for a in shapes],
            scratch_shapes=[pltpu.VMEM((rows, columns), F32), pltpu.VMEM((rows // NEAR, across), F32)],
        ),
        out_shape=shapes,
        name="project",
    )(place, *operands, *([small_weights] * 4), before, after, far)


def combine_body(wide, kept_ref, up_ref, down_ref, across_ref, ahead_ref, behind_ref):
    def summed(at, pieces):
        big = kept_ref[at][:, :wide]
        small = kept_ref[at][:, wide:]
        for piece in pieces:
            more_big, more_small = joined(piece, wide)
            big = big + more_big
            small = small + more_small
        return jnp.concatenate([big, small], axis=1)

    for out_ref, total in (
        (ahead_ref, summed(1, (up_ref[1], across_ref[0]))),
        (behind_ref, summed(2, (down_ref[1],))),
    ):
        big, little = split(total, wide)
        out_ref[:, :wide] = big
        out_ref[:, wide:] = little


def combine(kept, up, down, across):
    wide = kept.shape[2] - LANES

    def body(*refs):
        combine_body(wide, *refs)

    vmem = pl.BlockSpec(memory_space=pltpu.VMEM)
    shape = jax.ShapeDtypeStruct(kept.shape[1:], BF16)
    return pl.pallas_call(
        body, in_specs=[vmem] * 4, out_specs=[vmem] * 2, out_shape=[shape] * 2, name="combine"
    )(kept, up, down, across)


def deliver_body(kv_size, place_ref, weight_ref, left_ref, three_ref, right_ref, out_ref):
    own_rows = out_ref.shape[1]
    far_members = kv_size // NEAR_OUT
    pieces = [left_ref[0], left_ref[1], left_ref[2], three_ref[0], three_ref[1], three_ref[2], right_ref[0], right_ref[1]]
    for n, piece in enumerate(pieces):
        product = jnp.dot(piece, weight_ref[...], preferred_element_type=F32)
        for j in range(far_members):
            owner = (place_ref[0] + n - 4 + NEAR_OUT * (j - 2) + kv_size) % kv_size
            out_ref[owner] = product[j * own_rows : (j + 1) * own_rows].astype(BF16)


def deliver(place, w_out, left, three, right, kv_size, own_rows):
    smem = pl.BlockSpec(memory_space=pltpu.SMEM)
    vmem = pl.BlockSpec(memory_space=pltpu.VMEM)

    def body(*refs):
        deliver_body(kv_size, *refs)

    return pl.pallas_call(
        body,
        in_specs=[smem] + [vmem] * 4,
        out_specs=vmem,
        out_shape=jax.ShapeDtypeStruct((kv_size, own_rows, w_out.shape[1]), BF16),
        name="deliver",
    )(place, w_out, left, three, right)


def propose_body(
    span_size, total_heads, model_width, shard_ref, rate_ref, gain_ref, kept_ref, up_ref, down_ref, ahead_ref, behind_ref, state_ref, out_ref
):
    rows = kept_ref.shape[1]
    seq_count, heads_here, depth = state_ref.shape[0], state_ref.shape[1], state_ref.shape[2]
    wide = heads_here * depth

    def total(at, size):
        summed = kept_ref[0, :, at : at + size]
        for piece in (up_ref[0], down_ref[0], ahead_ref[...], behind_ref[...]):
            summed = summed + piece[:, at : at + size].astype(F32)
        return summed

    small = total(4 * wide, LANES)
    small = small + pltpu.roll(small, HALF, 1)
    lane = lax.broadcasted_iota(jnp.int32, small.shape, 1)

    def column(at):
        return jnp.sum(jnp.where(lane == at, small, F32(0.0)), axis=1, keepdims=True)

    inverse = lax.rsqrt(column(HALF - 1) / model_width + EPS)
    row = lax.broadcasted_iota(jnp.int32, (rows, 1), 0)
    place = row % span_size
    out_gain = gain_ref[...].astype(F32)

    def back(values, by):
        moved = pltpu.roll(values, by, 0)
        return jnp.where(place >= by, moved, F32(0.0))

    def dots(left, right):
        return jnp.sum(left * right, axis=1, keepdims=True)

    def unit(vectors):
        return vectors * lax.rsqrt(dots(vectors, vectors) + EPS)

    def over_lanes(values):
        return jnp.broadcast_to(values, (rows, depth))

    for head in range(heads_here):
        first = head * depth
        queries = unit(total(first, depth) * inverse) * F32(depth ** (-0.5))
        keys = unit(total(wide + first, depth) * inverse)
        values = total(2 * wide + first, depth) * inverse
        gate = total(3 * wide + first, depth) * inverse
        head_at = shard_ref[0] * heads_here + head
        beta = over_lanes(jax.nn.sigmoid(column(head_at) * inverse))
        logit = over_lanes(column(total_heads + head_at) * inverse)
        softplus = jnp.maximum(logit, F32(0.0)) + jnp.log1p(jnp.exp(-jnp.abs(logit)))
        log_decay = -rate_ref[head] * softplus
        cumulative = log_decay
        for by in range(1, span_size):
            cumulative = cumulative + back(log_decay, by)
        grown = jnp.exp(cumulative)
        moved_keys = [keys] + [back(keys, by) for by in range(1, span_size)]
        within = [None] + [
            jnp.where(place >= by, jnp.exp(jnp.where(place >= by, cumulative - back(cumulative, by), F32(0.0))), F32(0.0))
            for by in range(1, span_size)
        ]
        lower = [None] + [beta * dots(keys, moved_keys[by]) * within[by] for by in range(1, span_size)]
        pushed = beta * values
        weighted = beta * grown * keys
        for step in range(1, span_size):
            at_step = place == step
            push_less = jnp.zeros_like(pushed)
            weight_less = jnp.zeros_like(weighted)
            for by in range(1, step + 1):
                push_less = push_less + lower[by] * back(pushed, by)
                weight_less = weight_less + lower[by] * back(weighted, by)
            pushed = pushed - jnp.where(at_step, push_less, F32(0.0))
            weighted = weighted - jnp.where(at_step, weight_less, F32(0.0))
        left = jnp.concatenate([weighted, queries * grown], axis=0)
        sequence = lax.broadcasted_iota(jnp.int32, (2 * rows, 1), 0) % rows // span_size
        read = jnp.zeros((2 * rows, depth), F32)
        for seq in range(seq_count):
            term = jnp.dot(left, state_ref[seq, head], precision=lax.Precision.HIGHEST, preferred_element_type=F32)
            read = jnp.where(sequence == seq, term, read)
        corrections = pushed - read[:rows]
        outputs = read[rows:] + dots(queries, keys) * corrections
        for by in range(1, span_size):
            outputs = outputs + dots(queries, moved_keys[by]) * within[by] * back(corrections, by)
        scale = lax.rsqrt(dots(outputs, outputs) / depth + EPS)
        out_ref[:, first : first + depth] = (outputs * scale * out_gain * (gate * jax.nn.sigmoid(gate))).astype(BF16)


def propose(shard_tp, decay_rate, out_gain, terms, carried, span_size, total_heads, model_width):
    def body(*refs):
        propose_body(span_size, total_heads, model_width, *refs)

    smem = pl.BlockSpec(memory_space=pltpu.SMEM)
    vmem = pl.BlockSpec(memory_space=pltpu.VMEM)
    wide = carried.shape[1] * carried.shape[2]
    return pl.pallas_call(
        body,
        in_specs=[smem, smem] + [vmem] * 7,
        out_specs=vmem,
        out_shape=jax.ShapeDtypeStruct((terms[0].shape[1], wide), BF16),
        name="propose",
    )(shard_tp.reshape(1), decay_rate, out_gain.reshape(1, -1), *terms, carried)


def shards(
    tokens,
    norm_gain,
    w_query,
    w_key,
    w_value,
    w_gate,
    w_beta,
    w_decay,
    decay_rate,
    out_gain,
    w_out,
    state,
    prev_keys,
    prev_values,
    prev_beta,
    prev_logdecay,
    accepted,
    kv_size,
    tp_size,
):
    seq_count, heads_here = state.shape[0], state.shape[1]
    span_size = prev_keys.shape[1]
    own_rows = seq_count * span_size
    columns = tokens.shape[1]
    model_width, total_heads = w_beta.shape
    shard_kv = lax.axis_index("kv")
    shard_tp = lax.axis_index("tp")
    window = (shard_kv + jnp.arange(-1, NEAR - 1)) % kv_size
    place = jnp.concatenate([shard_kv[None], window]).astype(jnp.int32)
    weights = [w_query, w_key, w_value, w_gate]
    gain = norm_gain[None, :]

    to_next, to_previous = pack(place, tokens, gain, weights, own_rows)
    before = shift(to_next, kv_size, 1)
    after = shift(to_previous, kv_size, -1)
    far = shift(after[: to_next.shape[0]], kv_size, -1)

    carried = replay(state, prev_keys, prev_values, prev_beta, prev_logdecay, accepted)
    small_weights = jnp.concatenate(
        [w_beta, w_decay, jnp.zeros((model_width, LANES - 2 * total_heads), w_beta.dtype)], axis=1
    )
    up, down, across, kept = project(place, tokens, gain, weights, small_weights, before, after, far, own_rows)
    up = shift(up, kv_size, NEAR)
    down = shift(down, kv_size, -NEAR)
    across = shift(across, kv_size, 2 * NEAR)
    ahead, behind = combine(kept, up, down, across)
    ahead = shift(ahead, kv_size, 2 * NEAR)
    behind = shift(behind, kv_size, -2 * NEAR)
    terms = (kept, up, down, ahead, behind)
    hidden = propose(shard_tp, decay_rate, out_gain, terms, carried, span_size, total_heads, model_width)

    below = shift(hidden, kv_size, NEAR_OUT)
    above = shift(hidden, kv_size, -NEAR_OUT)
    opposite = shift(below, kv_size, NEAR_OUT)
    block = jnp.concatenate([opposite, below, hidden, above], axis=0)
    left = shift(block, kv_size, 1)
    right = shift(block, kv_size, -1)
    three = jnp.stack([left, block, right])
    near_left = shift(three, kv_size, 3)
    near_right = shift(three[:2], kv_size, -3)
    partial = deliver(place, w_out, near_left, three, near_right, kv_size, own_rows)
    partial = partial.reshape(kv_size * own_rows, -1)
    exchanged = lax.all_to_all(partial, "tp", 0, 0, tiled=True)
    exchanged = exchanged.reshape(tp_size, -1, exchanged.shape[1])
    summed = jnp.sum(exchanged.astype(F32), axis=0).astype(BF16)
    mixed = lax.all_to_all(jnp.tile(summed, (tp_size, 1)), "tp", 0, 0, tiled=True)
    return (mixed, carried)


def solution(mesh):
    in_specs = (
        P("grp", "kv"),
        P("kv"),
        P("kv", "tp"),
        P("kv", "tp"),
        P("kv", "tp"),
        P("kv", "tp"),
        P(),
        P(),
        P("tp"),
        P(),
        P("tp", "kv"),
        P(("grp", "kv"), "tp", None, None),
        P(("grp", "kv"), None, "tp", None),
        P(("grp", "kv"), None, "tp", None),
        P(("grp", "kv"), None, "tp"),
        P(("grp", "kv"), None, "tp"),
        P(("grp", "kv")),
    )
    out_specs = (P("grp", "kv"), P(("grp", "kv"), "tp", None, None))

    def per_device(*arguments):
        return shards(*arguments, kv_size=mesh.shape["kv"], tp_size=mesh.shape["tp"])

    return jax.shard_map(per_device, mesh=mesh, in_specs=in_specs, out_specs=out_specs, check_vma=False)
```

```python
import jax
import jax.numpy as jnp
from jax import lax
from jax.experimental import pallas as pl
from jax.experimental.pallas import tpu as pltpu
from jax.sharding import PartitionSpec as P


EPS = 1e-06
WINDOW = (-1, 0, 1, 2)
JUMP = len(WINDOW)
NEAR_OUT = 8
AHEAD = (0, JUMP, -JUMP, 2 * JUMP, -2 * JUMP, 3 * JUMP, -3 * JUMP, 4 * JUMP)
GATHER = "near"
LANES = 128
HALF = LANES // 2
F32 = jnp.float32
BF16 = jnp.bfloat16


def near_memory(array):
    return pltpu.with_memory_space_constraint(array, pltpu.MemorySpace.VMEM)


def kernel(body, scalars, arrays, shapes, scratch=(), in_near=True, out_near=True):
    smem = pl.BlockSpec(memory_space=pltpu.SMEM)
    vmem = pl.BlockSpec(memory_space=pltpu.VMEM)
    kind = pltpu.VMEM if out_near else jax.ShapeDtypeStruct
    return pl.pallas_call(
        body,
        in_specs=[smem] * len(scalars) + [vmem] * len(arrays),
        out_specs=[vmem] * len(shapes),
        out_shape=[kind(shape, dtype) for shape, dtype in shapes],
        scratch_shapes=list(scratch),
    )(*scalars, *[near_memory(array) if in_near else array for array in arrays])


def shift(table, axis_size, by):
    return lax.ppermute(table, "kv", [(i, (i + by) % axis_size) for i in range(axis_size)])


def replay_body(keys_ref, values_ref, beta_ref, logdecay_ref, accepted_ref, state_ref, out_ref):
    seq = pl.program_id(0)
    heads_here, depth = state_ref.shape[1], state_ref.shape[2]
    span_size = keys_ref.shape[1] // heads_here
    for head in range(heads_here):
        carry = state_ref[0, head]
        for position in range(span_size):
            row = position * heads_here + head
            active = accepted_ref[seq] > position
            spot = seq * span_size * heads_here + row
            logdecay = jnp.where(active, logdecay_ref[spot], F32(0.0))
            strength = jnp.where(active, beta_ref[spot], F32(0.0))
            factor = jnp.exp(jnp.full((1, depth), logdecay, F32))
            key = keys_ref[0, row : row + 1, :]
            key = key * lax.rsqrt(jnp.sum(key * key, axis=-1, keepdims=True) + EPS)
            key_columns = jnp.transpose(jnp.broadcast_to(key, (depth, depth)))
            carry = factor * carry
            predicted = jnp.sum(key_columns * carry, axis=0, keepdims=True)
            update = strength * (values_ref[0, row : row + 1, :] - predicted)
            carry = carry + key_columns * update
        out_ref[0, head] = carry


def replay(state, prev_keys, prev_values, prev_beta, prev_logdecay, accepted):
    seq_count, heads_here, depth, _ = state.shape
    rows = prev_keys.shape[1] * heads_here
    keys = prev_keys.astype(F32).reshape(seq_count, rows, depth)
    values = prev_values.astype(F32).reshape(seq_count, rows, depth)
    row_spec = pl.BlockSpec((1, rows, depth), lambda b: (b, 0, 0))
    state_spec = pl.BlockSpec((1, heads_here, depth, depth), lambda b: (b, 0, 0, 0))
    smem = pl.BlockSpec(memory_space=pltpu.SMEM)
    return pl.pallas_call(
        replay_body,
        grid=(seq_count,),
        in_specs=[row_spec, row_spec, smem, smem, smem, state_spec],
        out_specs=state_spec,
        out_shape=jax.ShapeDtypeStruct(state.shape, F32),
        name="replay",
    )(keys, values, prev_beta.reshape(-1), prev_logdecay.reshape(-1), accepted, state)


def rows_for(wide_ref, device, kv_size, own_rows):
    owners = [(device + ahead + 2 * kv_size) % kv_size for ahead in AHEAD]
    pieces = [wide_ref[pl.ds(pl.multiple_of(owner * own_rows, 8), own_rows), :] for owner in owners]
    return jnp.concatenate(pieces, axis=0)


def side_by_side(rows):
    half = rows.shape[0] // 2
    return jnp.concatenate([rows[:half], rows[half:]], axis=1).astype(BF16)


def layout(columns, own_rows):
    weights_at = 0 if GATHER == "near" else columns
    gain_at = weights_at + 4 * columns
    rows_at = gain_at + 16
    return weights_at, gain_at, rows_at, len(AHEAD) * own_rows // 2


def pack_body(
    kv_size, own_rows, tokens_ref, gain_ref, wq_ref, wk_ref, wv_ref, wg_ref, wo_ref, next_ref, previous_ref, own_ref, wide_ref
):
    columns = gain_ref.shape[1]
    weights_at, gain_at, rows_at, half = layout(columns, own_rows)
    shard_kv = lax.axis_index("kv")
    wide_ref[...] = tokens_ref[...].astype(F32)
    own_ref[...] = rows_for(wide_ref, shard_kv, kv_size, own_rows)
    gain = jnp.concatenate([gain_ref[...]] * (wq_ref.shape[1] // columns), axis=1)
    gain = jnp.broadcast_to(gain, (16, wq_ref.shape[1]))
    for out_ref, stops in ((next_ref, (1,)), (previous_ref, (-2, -1))):
        if GATHER != "near":
            out_ref[:columns, :columns] = wo_ref[:columns, :]
            out_ref[:columns, columns:] = wo_ref[columns:, :]
        for j, weight_ref in enumerate((wq_ref, wk_ref, wv_ref, wg_ref)):
            out_ref[weights_at + j * columns : weights_at + (j + 1) * columns, :] = weight_ref[...]
        out_ref[gain_at:rows_at, :] = gain
        for at, stop in enumerate(stops):
            rows = side_by_side(rows_for(wide_ref, shard_kv + stop, kv_size, own_rows))
            out_ref[rows_at + at * half : rows_at + (at + 1) * half, :] = rows


def pack(tokens, gain, weights, w_out, kv_size, own_rows):
    columns = tokens.shape[1]
    _, _, rows_at, half = layout(columns, own_rows)
    wide = weights[0].shape[1]

    def body(*refs):
        pack_body(kv_size, own_rows, *refs)

    shapes = [((rows_at + stops * half, wide), BF16) for stops in (1, 2)] + [((2 * half, columns), F32)]
    scratch = [pltpu.VMEM(tokens.shape, F32)]
    return kernel(body, [], [tokens, gain, *weights, w_out], shapes, scratch, in_near=False)


def split(values, wide):
    small = values[:, wide:]
    lane = lax.broadcasted_iota(jnp.int32, small.shape, 1)
    coarse = small.astype(BF16).astype(F32)
    rest = pltpu.roll(small - coarse, HALF, 1)
    return values[:, :wide].astype(BF16), jnp.where(lane < HALF, coarse, rest).astype(BF16)


def joined(terms, wide):
    small = terms[:, wide:].astype(F32)
    lane = lax.broadcasted_iota(jnp.int32, small.shape, 1)
    small = jnp.where(lane < HALF, small + pltpu.roll(small, HALF, 1), F32(0.0))
    return terms[:, :wide].astype(F32), small


def project_body(
    kv_size, own_rows, columns, own_rows_ref, small_ref, own_ref, before_ref, after_ref, after2_ref, up_ref, down_ref, across_ref, kept_ref, sums_ref
):
    wide = own_ref.shape[1]
    weights_at, gain_at, rows_at, half = layout(columns, own_rows)
    shard_kv = lax.axis_index("kv")

    def taken(pay_ref, at):
        weights = [pay_ref[weights_at + j * columns : weights_at + (j + 1) * columns, :] for j in range(4)]
        gain = pay_ref[gain_at:rows_at, :columns].astype(F32)[:1]
        if at is None:
            return own_rows_ref[...], gain, weights
        both = pay_ref[rows_at + at * half : rows_at + (at + 1) * half, :].astype(F32)
        return jnp.concatenate([both[:, :columns], both[:, columns:]], axis=0), gain, weights

    parts = [taken(before_ref, 0), taken(own_ref, None), taken(after_ref, 1), taken(after2_ref, 0)]
    sums = [None] * 4
    small = None
    squares = None
    for at, (widened, gain, weights) in enumerate(parts):
        term = jnp.sum(widened * widened, axis=1, keepdims=True)
        squares = term if squares is None else squares + term
        scaled = (widened * gain).astype(BF16)
        for j in range(4):
            term = jnp.dot(scaled, weights[j], preferred_element_type=F32)
            sums[j] = term if sums[j] is None else sums[j] + term
        small_at = pl.multiple_of((shard_kv + WINDOW[at] + kv_size) % kv_size * columns, columns)
        term = jnp.dot(scaled, small_ref[pl.ds(small_at, columns), :], preferred_element_type=F32)
        small = term if small is None else small + term
    lane = lax.broadcasted_iota(jnp.int32, small.shape, 1)
    small = jnp.where(lane == HALF - 1, squares, small)
    for j in range(4):
        sums_ref[:, j * wide : (j + 1) * wide] = sums[j]
    sums_ref[:, 4 * wide :] = small

    def block(ahead):
        start = AHEAD.index(ahead) * own_rows
        return sums_ref[start : start + own_rows, :]

    for out_ref, at, ahead in (
        (up_ref, 0, JUMP),
        (up_ref, 1, 3 * JUMP),
        (down_ref, 0, -JUMP),
        (down_ref, 1, -3 * JUMP),
        (across_ref, 0, 4 * JUMP),
    ):
        big, little = split(block(ahead), 4 * wide)
        out_ref[at, :, : 4 * wide] = big
        out_ref[at, :, 4 * wide :] = little
    for at, ahead in enumerate((0, 2 * JUMP, -2 * JUMP)):
        kept_ref[at] = block(ahead)


def project(own_rows_wide, small_weights, packets, kv_size, own_rows):
    columns = own_rows_wide.shape[1]
    across = 4 * packets[0].shape[1] + LANES
    shapes = [((count, own_rows, across), BF16) for count in (2, 2, 1)] + [((3, own_rows, across), F32)]

    def body(*refs):
        project_body(kv_size, own_rows, columns, *refs)

    scratch = [pltpu.VMEM((len(AHEAD) * own_rows, across), F32)]
    return kernel(body, [], [own_rows_wide, small_weights, *packets], shapes, scratch)


def combine_body(wide, kept_ref, up_ref, down_ref, across_ref, carried_ref, ahead_ref, behind_ref):
    del carried_ref
    for at, pieces, out_ref in ((1, (up_ref[1], across_ref[0]), ahead_ref), (2, (down_ref[1],), behind_ref)):
        big = kept_ref[at][:, :wide]
        small = kept_ref[at][:, wide:]
        for piece in pieces:
            more_big, more_small = joined(piece, wide)
            big = big + more_big
            small = small + more_small
        big, little = split(jnp.concatenate([big, small], axis=1), wide)
        out_ref[:, :wide] = big
        out_ref[:, wide:] = little


def combine(kept, up, down, across, carried):
    wide = kept.shape[2] - LANES

    def body(*refs):
        combine_body(wide, *refs)

    shapes = [(kept.shape[1:], BF16)] * 2
    return kernel(body, [], [kept, up, down, across, carried], shapes)


def deliver_body(*refs):
    *row_refs, wo_ref, before_ref, after_ref, after2_ref, out_ref = refs
    rows = jnp.concatenate([ref[...] for ref in row_refs], axis=0)
    columns = wo_ref.shape[1]
    for at, packet_ref in enumerate((before_ref, None, after_ref, after2_ref)):
        if packet_ref is None:
            weight = wo_ref[...]
        else:
            weight = jnp.concatenate([packet_ref[:columns, :columns], packet_ref[:columns, columns:]], axis=0)
        product = jnp.dot(rows, weight, preferred_element_type=F32)
        out_ref[:, at * columns : (at + 1) * columns] = product.astype(BF16)


def deliver(pieces, w_out, packets):
    shape = (sum(piece.shape[0] for piece in pieces), JUMP * w_out.shape[1])
    (partial,) = kernel(deliver_body, [], [*pieces, w_out, *packets], [(shape, BF16)])
    return partial


def deliver_near_body(kv_size, weight_ref, left_ref, three_ref, right_ref, out_ref):
    shard_kv = lax.axis_index("kv")
    own_rows = out_ref.shape[1]
    far_members = kv_size // NEAR_OUT
    pieces = [left_ref[0], left_ref[1], left_ref[2], three_ref[0], three_ref[1], three_ref[2], right_ref[0], right_ref[1]]
    for n, piece in enumerate(pieces):
        product = jnp.dot(piece, weight_ref[...], preferred_element_type=F32)
        for j in range(far_members):
            owner = (shard_kv + n - 4 + NEAR_OUT * (j - 2) + kv_size) % kv_size
            out_ref[owner] = product[j * own_rows : (j + 1) * own_rows].astype(BF16)


def deliver_near(w_out, left, three, right, kv_size, own_rows):
    def body(*refs):
        deliver_near_body(kv_size, *refs)

    shape = (kv_size, own_rows, w_out.shape[1])
    (partial,) = kernel(body, [], [w_out, left, three, right], [(shape, BF16)])
    return partial


def reduce_all_body(terms_ref, out_ref):
    total = terms_ref[0].astype(F32)
    for member in range(1, terms_ref.shape[0]):
        total = total + terms_ref[member].astype(F32)
    for member in range(terms_ref.shape[0]):
        out_ref[member] = total.astype(BF16)


def reduce_all(terms):
    (copies,) = kernel(reduce_all_body, [], [terms], [(terms.shape, BF16)])
    return copies


def stack_body(*refs):
    out_ref = refs[-1]
    for at, ref in enumerate(refs[:-1]):
        out_ref[at] = ref[...]


def stacked(pieces):
    (out,) = kernel(stack_body, [], pieces, [((len(pieces), *pieces[0].shape), BF16)])
    return out


def reduce_body(terms_ref, *out_refs):
    columns = out_refs[0].shape[1]
    for at, out_ref in enumerate(out_refs):
        total = terms_ref[0, :, at * columns : (at + 1) * columns].astype(F32)
        for member in range(1, terms_ref.shape[0]):
            total = total + terms_ref[member, :, at * columns : (at + 1) * columns].astype(F32)
        out_ref[...] = total.astype(BF16)


def reduce_terms(terms):
    _, rows, wide = terms.shape
    return kernel(reduce_body, [], [terms], [((rows, wide // JUMP), BF16)] * JUMP)


def spread_body(*refs):
    out_ref = refs[-1]
    for at, piece_ref in enumerate(refs[:-1]):
        for member in range(out_ref.shape[0]):
            out_ref[member, at] = piece_ref[...]


def spread(pieces, copies):
    (out,) = kernel(spread_body, [], pieces, [((copies, len(pieces), *pieces[0].shape), BF16)])
    return out


def settle_body(blocks_ref, out_ref):
    shard_kv = lax.axis_index("kv")
    kv_size = blocks_ref.shape[0]
    for n in range(kv_size):
        if GATHER == "exchange":
            owner = (shard_kv + n % JUMP + JUMP - WINDOW[-1]) % JUMP + n // JUMP * JUMP
        else:
            owner = (shard_kv + n + 2 * kv_size - WINDOW[-1] - 3 * JUMP) % kv_size
        out_ref[owner] = blocks_ref[n]


def settle(blocks):
    (out,) = kernel(settle_body, [], [blocks], [(blocks.shape, BF16)], out_near=False)
    return out


def propose_body(
    span_size, total_heads, model_width, rate_ref, gain_ref, kept_ref, up_ref, down_ref, ahead_ref, behind_ref, state_ref, out_ref
):
    rows = kept_ref.shape[1]
    seq_count, heads_here, depth = state_ref.shape[0], state_ref.shape[1], state_ref.shape[2]
    wide = heads_here * depth

    def total(at, size):
        summed = kept_ref[0, :, at : at + size]
        for piece in (up_ref[0], down_ref[0], ahead_ref[...], behind_ref[...]):
            summed = summed + piece[:, at : at + size].astype(F32)
        return summed

    small = total(4 * wide, LANES)
    small = small + pltpu.roll(small, HALF, 1)
    lane = lax.broadcasted_iota(jnp.int32, small.shape, 1)

    def column(at):
        return jnp.sum(jnp.where(lane == at, small, F32(0.0)), axis=1, keepdims=True)

    inverse = lax.rsqrt(column(HALF - 1) / model_width + EPS)
    row = lax.broadcasted_iota(jnp.int32, (rows, 1), 0)
    place = row % span_size
    out_gain = gain_ref[...].astype(F32)

    def back(values, by):
        moved = pltpu.roll(values, by, 0)
        return jnp.where(place >= by, moved, F32(0.0))

    def dots(left, right):
        return jnp.sum(left * right, axis=1, keepdims=True)

    def unit(vectors):
        return vectors * lax.rsqrt(dots(vectors, vectors) + EPS)

    def over_lanes(values):
        return jnp.broadcast_to(values, (rows, depth))

    for head in range(heads_here):
        first = head * depth
        queries = unit(total(first, depth) * inverse) * F32(depth ** (-0.5))
        keys = unit(total(wide + first, depth) * inverse)
        values = total(2 * wide + first, depth) * inverse
        gate = total(3 * wide + first, depth) * inverse
        head_at = lax.axis_index("tp") * heads_here + head
        beta = over_lanes(jax.nn.sigmoid(column(head_at) * inverse))
        logit = over_lanes(column(total_heads + head_at) * inverse)
        softplus = jnp.maximum(logit, F32(0.0)) + jnp.log1p(jnp.exp(-jnp.abs(logit)))
        log_decay = -rate_ref[head] * softplus
        cumulative = log_decay
        for by in range(1, span_size):
            cumulative = cumulative + back(log_decay, by)
        grown = jnp.exp(cumulative)
        moved_keys = [keys] + [back(keys, by) for by in range(1, span_size)]
        within = [None] + [
            jnp.where(place >= by, jnp.exp(jnp.where(place >= by, cumulative - back(cumulative, by), F32(0.0))), F32(0.0))
            for by in range(1, span_size)
        ]
        lower = [None] + [beta * dots(keys, moved_keys[by]) * within[by] for by in range(1, span_size)]
        pushed = beta * values
        weighted = beta * grown * keys
        for step in range(1, span_size):
            at_step = place == step
            push_less = jnp.zeros_like(pushed)
            weight_less = jnp.zeros_like(weighted)
            for by in range(1, step + 1):
                push_less = push_less + lower[by] * back(pushed, by)
                weight_less = weight_less + lower[by] * back(weighted, by)
            pushed = pushed - jnp.where(at_step, push_less, F32(0.0))
            weighted = weighted - jnp.where(at_step, weight_less, F32(0.0))
        left = jnp.concatenate([weighted, queries * grown], axis=0)
        sequence = lax.broadcasted_iota(jnp.int32, (2 * rows, 1), 0) % rows // span_size
        read = jnp.zeros((2 * rows, depth), F32)
        for seq in range(seq_count):
            term = jnp.dot(left, state_ref[seq, head], precision=lax.Precision.HIGHEST, preferred_element_type=F32)
            read = jnp.where(sequence == seq, term, read)
        corrections = pushed - read[:rows]
        outputs = read[rows:] + dots(queries, keys) * corrections
        for by in range(1, span_size):
            outputs = outputs + dots(queries, moved_keys[by]) * within[by] * back(corrections, by)
        scale = lax.rsqrt(dots(outputs, outputs) / depth + EPS)
        finished = (outputs * scale * out_gain * (gate * jax.nn.sigmoid(gate))).astype(BF16)
        for copy in range(out_ref.shape[0] // rows):
            out_ref[copy * rows : (copy + 1) * rows, first : first + depth] = finished


def propose(decay_rate, out_gain, terms, carried, span_size, total_heads, model_width, copies):
    def body(*refs):
        propose_body(span_size, total_heads, model_width, *refs)

    wide = carried.shape[1] * carried.shape[2]
    shape = (copies * terms[0].shape[1], wide)
    operands = [out_gain.reshape(1, -1), *terms, carried]
    (hidden,) = kernel(body, [decay_rate], operands, [(shape, BF16)])
    return hidden


def shards(
    tokens,
    norm_gain,
    w_query,
    w_key,
    w_value,
    w_gate,
    w_beta,
    w_decay,
    decay_rate,
    out_gain,
    w_out,
    state,
    prev_keys,
    prev_values,
    prev_beta,
    prev_logdecay,
    accepted,
    kv_size,
    tp_size,
):
    seq_count = state.shape[0]
    span_size = prev_keys.shape[1]
    own_rows = seq_count * span_size
    model_width, total_heads = w_beta.shape
    weights = [w_query, w_key, w_value, w_gate]
    to_next, to_previous, own_rows_wide = pack(tokens, norm_gain[None, :], weights, w_out, kv_size, own_rows)
    before = shift(to_next, kv_size, 1)
    after = shift(to_previous, kv_size, -1)
    after2 = shift(after[: to_next.shape[0]], kv_size, -1)

    carried = replay(state, prev_keys, prev_values, prev_beta, prev_logdecay, accepted)
    small_weights = jnp.concatenate(
        [w_beta, w_decay, jnp.zeros((model_width, LANES - 2 * total_heads), w_beta.dtype)], axis=1
    )
    packets = (to_next, before, after, after2)
    up, down, across, kept = project(own_rows_wide, small_weights, packets, kv_size, own_rows)
    across = shift(across, kv_size, 2 * JUMP)
    up = shift(up, kv_size, JUMP)
    down = shift(down, kv_size, -JUMP)
    ahead, behind = combine(kept, up, down, across, carried)
    ahead = shift(ahead, kv_size, 2 * JUMP)
    behind = shift(behind, kv_size, -2 * JUMP)
    terms = (kept, up, down, ahead, behind)
    members = kv_size // JUMP
    copies = members if GATHER == "exchange" else 1
    hidden = propose(decay_rate, out_gain, terms, carried, span_size, total_heads, model_width, copies)

    if GATHER == "near":
        below = shift(hidden, kv_size, NEAR_OUT)
        above = shift(hidden, kv_size, -NEAR_OUT)
        opposite = shift(below, kv_size, NEAR_OUT)
        block = stacked([opposite, below, hidden, above]).reshape(4 * own_rows, -1)
        left = shift(block, kv_size, 1)
        right = shift(block, kv_size, -1)
        three = stacked([left, block, right])
        near_left = shift(three, kv_size, 3)
        near_right = shift(three[:2], kv_size, -3)
        partial = deliver_near(w_out, near_left, three, near_right, kv_size, own_rows)
        exchanged = lax.all_to_all(partial.reshape(kv_size * own_rows, -1), "tp", 0, 0, tiled=True)
        copies = reduce_all(exchanged.reshape(tp_size, -1, exchanged.shape[1]))
        mixed = lax.all_to_all(copies.reshape(exchanged.shape), "tp", 0, 0, tiled=True)
        return (mixed, carried)
    if GATHER == "exchange":
        groups = [list(range(first, kv_size, JUMP)) for first in range(JUMP)]
        pieces = (lax.all_to_all(hidden, "kv", 0, 0, tiled=True, axis_index_groups=groups),)
    else:
        below = shift(hidden, kv_size, JUMP)
        above = shift(hidden, kv_size, -JUMP)
        three = jnp.concatenate([below, hidden, above], axis=0)
        low = shift(three[own_rows:], kv_size, 3 * JUMP)
        high = shift(three, kv_size, -3 * JUMP)
        pieces = (low, three, high)
    partial = deliver(pieces, w_out, (before, after, after2))
    exchanged = lax.all_to_all(partial, "tp", 0, 0, tiled=True)
    finished = reduce_terms(exchanged.reshape(tp_size, own_rows, -1))
    landed = [
        piece if offset == 0 else shift(piece, kv_size, offset) for offset, piece in zip(WINDOW, finished)
    ][::-1]
    copies = spread(landed, tp_size).reshape(kv_size * own_rows, -1)
    mixed = lax.all_to_all(copies, "tp", 0, 0, tiled=True)
    mixed = settle(mixed.reshape(kv_size, own_rows, -1)).reshape(kv_size * own_rows, -1)
    return (mixed, carried)


def solution(mesh):
    in_specs = (
        P("grp", "kv"),
        P("kv"),
        P("kv", "tp"),
        P("kv", "tp"),
        P("kv", "tp"),
        P("kv", "tp"),
        P(),
        P(),
        P("tp"),
        P(),
        P("tp", "kv"),
        P(("grp", "kv"), "tp", None, None),
        P(("grp", "kv"), None, "tp", None),
        P(("grp", "kv"), None, "tp", None),
        P(("grp", "kv"), None, "tp"),
        P(("grp", "kv"), None, "tp"),
        P(("grp", "kv")),
    )
    out_specs = (P("grp", "kv"), P(("grp", "kv"), "tp", None, None))

    def per_device(*arguments):
        return shards(*arguments, kv_size=mesh.shape["kv"], tp_size=mesh.shape["tp"])

    return jax.shard_map(per_device, mesh=mesh, in_specs=in_specs, out_specs=out_specs, check_vma=False)
```

```python
import jax
import jax.numpy as jnp
from jax import lax
from jax.experimental import pallas as pl
from jax.experimental.pallas import tpu as pltpu
from jax.sharding import PartitionSpec as P


EPS = 1e-06
WINDOW = (-1, 0, 1, 2)
JUMP = len(WINDOW)
AHEAD = (0, JUMP, -JUMP, 2 * JUMP, -2 * JUMP, 3 * JUMP, -3 * JUMP, 4 * JUMP)
LANES = 128
HALF = LANES // 2
F32 = jnp.float32
BF16 = jnp.bfloat16


def near_memory(array):
    return pltpu.with_memory_space_constraint(array, pltpu.MemorySpace.VMEM)


def kernel(body, scalars, arrays, shapes, scratch=(), in_near=True, out_near=True):
    smem = pl.BlockSpec(memory_space=pltpu.SMEM)
    vmem = pl.BlockSpec(memory_space=pltpu.VMEM)
    kind = pltpu.VMEM if out_near else jax.ShapeDtypeStruct
    return pl.pallas_call(
        body,
        in_specs=[smem] * len(scalars) + [vmem] * len(arrays),
        out_specs=[vmem] * len(shapes),
        out_shape=[kind(shape, dtype) for shape, dtype in shapes],
        scratch_shapes=list(scratch),
    )(*scalars, *[near_memory(array) if in_near else array for array in arrays])


def shift(table, axis_size, by):
    return lax.ppermute(table, "kv", [(i, (i + by) % axis_size) for i in range(axis_size)])


def replay_body(beta_ref, logdecay_ref, accepted_ref, keys_ref, values_ref, state_ref, out_ref, rows_ref):
    seq_count, span_size, heads_here, depth = keys_ref.shape
    rows_ref[...] = jnp.zeros(rows_ref.shape, F32)

    def one(seq, carry):
        for position in range(span_size):
            first = position * heads_here
            keys = keys_ref[seq, position].astype(F32)
            keys = keys * lax.rsqrt(jnp.sum(keys * keys, axis=-1, keepdims=True) + EPS)
            rows_ref[first : first + heads_here, :] = keys
        key_columns = jnp.transpose(rows_ref[...])
        for head in range(heads_here):
            state = state_ref[seq, head]
            for position in range(span_size):
                row = position * heads_here + head
                spot = seq * span_size * heads_here + row
                active = accepted_ref[seq] > position
                logdecay = jnp.where(active, logdecay_ref[spot], F32(0.0))
                strength = jnp.where(active, beta_ref[spot], F32(0.0))
                column = jnp.broadcast_to(key_columns[:, row : row + 1], (depth, depth))
                state = jnp.exp(jnp.full((1, depth), logdecay, F32)) * state
                predicted = jnp.sum(column * state, axis=0, keepdims=True)
                value = values_ref[seq, position].astype(F32)[head : head + 1]
                state = state + column * (strength * (value - predicted))
            out_ref[seq, head] = state
        return carry

    lax.fori_loop(0, seq_count, one, 0)


def replay(state, prev_keys, prev_values, beta, logdecay, accepted):
    rows = -(-prev_keys.shape[1] * prev_keys.shape[2] // 8) * 8
    scratch = [pltpu.VMEM((rows, state.shape[-1]), F32)]
    scalars = [beta, logdecay, accepted]
    (carried,) = kernel(replay_body, scalars, [prev_keys, prev_values, state], [(state.shape, F32)], scratch)
    return carried


def rows_for(wide_ref, device, kv_size, own_rows):
    owners = [(device + ahead + 2 * kv_size) % kv_size for ahead in AHEAD]
    pieces = [wide_ref[pl.ds(pl.multiple_of(owner * own_rows, 8), own_rows), :] for owner in owners]
    return jnp.concatenate(pieces, axis=0)


def side_by_side(rows):
    half = rows.shape[0] // 2
    return jnp.concatenate([rows[:half], rows[half:]], axis=1).astype(BF16)


def layout(columns, own_rows):
    weights_at = columns
    gain_at = weights_at + 4 * columns
    rows_at = gain_at + 16
    return weights_at, gain_at, rows_at, len(AHEAD) * own_rows // 2


def pack_body(
    kv_size, own_rows, tokens_ref, gain_ref, wq_ref, wk_ref, wv_ref, wg_ref, wo_ref, next_ref, previous_ref, own_ref, wide_ref
):
    columns = gain_ref.shape[1]
    weights_at, gain_at, rows_at, half = layout(columns, own_rows)
    shard_kv = lax.axis_index("kv")
    wide_ref[...] = tokens_ref[...].astype(F32)
    own_ref[...] = rows_for(wide_ref, shard_kv, kv_size, own_rows)
    gain = jnp.concatenate([gain_ref[...]] * (wq_ref.shape[1] // columns), axis=1)
    gain = jnp.broadcast_to(gain, (16, wq_ref.shape[1]))
    for out_ref, stops in ((next_ref, (1,)), (previous_ref, (-2, -1))):
        out_ref[:columns, :columns] = wo_ref[:columns, :]
        out_ref[:columns, columns:] = wo_ref[columns:, :]
        for j, weight_ref in enumerate((wq_ref, wk_ref, wv_ref, wg_ref)):
            out_ref[weights_at + j * columns : weights_at + (j + 1) * columns, :] = weight_ref[...]
        out_ref[gain_at:rows_at, :] = gain
        for at, stop in enumerate(stops):
            rows = side_by_side(rows_for(wide_ref, shard_kv + stop, kv_size, own_rows))
            out_ref[rows_at + at * half : rows_at + (at + 1) * half, :] = rows


def pack(tokens, gain, weights, w_out, kv_size, own_rows):
    columns = tokens.shape[1]
    _, _, rows_at, half = layout(columns, own_rows)
    wide = weights[0].shape[1]

    def body(*refs):
        pack_body(kv_size, own_rows, *refs)

    shapes = [((rows_at + stops * half, wide), BF16) for stops in (1, 2)] + [((2 * half, columns), F32)]
    scratch = [pltpu.VMEM(tokens.shape, F32)]
    return kernel(body, [], [tokens, gain, *weights, w_out], shapes, scratch, in_near=False)


def split(values, wide):
    small = values[:, wide:]
    lane = lax.broadcasted_iota(jnp.int32, small.shape, 1)
    coarse = small.astype(BF16).astype(F32)
    rest = pltpu.roll(small - coarse, HALF, 1)
    return values[:, :wide].astype(BF16), jnp.where(lane < HALF, coarse, rest).astype(BF16)


def joined(terms, wide):
    small = terms[:, wide:].astype(F32)
    lane = lax.broadcasted_iota(jnp.int32, small.shape, 1)
    small = jnp.where(lane < HALF, small + pltpu.roll(small, HALF, 1), F32(0.0))
    return terms[:, :wide].astype(F32), small


def project_body(
    kv_size,
    own_rows,
    columns,
    own_rows_ref,
    small_ref,
    own_ref,
    before_ref,
    after_ref,
    after2_ref,
    up_ref,
    down_ref,
    across_ref,
    kept_ref,
    w_out_ref,
    sums_ref,
):
    for at, packet_ref in enumerate((before_ref, own_ref, after_ref, after2_ref)):
        for part in range(w_out_ref.shape[0] // columns):
            piece = packet_ref[:columns, part * columns : (part + 1) * columns]
            w_out_ref[part * columns : (part + 1) * columns, at * columns : (at + 1) * columns] = piece
    wide = own_ref.shape[1]
    weights_at, gain_at, rows_at, half = layout(columns, own_rows)
    shard_kv = lax.axis_index("kv")

    def taken(pay_ref, at):
        weights = [pay_ref[weights_at + j * columns : weights_at + (j + 1) * columns, :] for j in range(4)]
        gain = pay_ref[gain_at:rows_at, :columns].astype(F32)[:1]
        if at is None:
            return own_rows_ref[...], gain, weights
        both = pay_ref[rows_at + at * half : rows_at + (at + 1) * half, :].astype(F32)
        return jnp.concatenate([both[:, :columns], both[:, columns:]], axis=0), gain, weights

    parts = [taken(before_ref, 0), taken(own_ref, None), taken(after_ref, 1), taken(after2_ref, 0)]
    sums = [None] * 4
    small = None
    squares = None
    for at, (widened, gain, weights) in enumerate(parts):
        term = jnp.sum(widened * widened, axis=1, keepdims=True)
        squares = term if squares is None else squares + term
        scaled = (widened * gain).astype(BF16)
        for j in range(4):
            term = jnp.dot(scaled, weights[j], preferred_element_type=F32)
            sums[j] = term if sums[j] is None else sums[j] + term
        small_at = pl.multiple_of((shard_kv + WINDOW[at] + kv_size) % kv_size * columns, columns)
        term = lax.dot_general(
            scaled, small_ref[:, pl.ds(small_at, columns)], (((1,), (1,)), ((), ())), preferred_element_type=F32
        )
        small = term if small is None else small + term
    for j in range(4):
        sums_ref[:, j * wide : (j + 1) * wide] = sums[j]
    lane = lax.broadcasted_iota(jnp.int32, (small.shape[0], LANES), 1)
    sums_ref[:, 4 * wide :] = jnp.where(lane == HALF - 1, squares, F32(0.0))
    sums_ref[:, 4 * wide : 4 * wide + small.shape[1]] = small

    def block(ahead):
        start = AHEAD.index(ahead) * own_rows
        return sums_ref[start : start + own_rows, :]

    for out_ref, at, ahead in (
        (up_ref, 0, JUMP),
        (up_ref, 1, 3 * JUMP),
        (down_ref, 0, -JUMP),
        (down_ref, 1, -3 * JUMP),
        (across_ref, 0, 4 * JUMP),
    ):
        big, little = split(block(ahead), 4 * wide)
        out_ref[at, :, : 4 * wide] = big
        out_ref[at, :, 4 * wide :] = little
    for at, ahead in enumerate((0, 2 * JUMP, -2 * JUMP)):
        kept_ref[at] = block(ahead)


def project(own_rows_wide, small_weights, packets, kv_size, own_rows):
    columns = own_rows_wide.shape[1]
    across = 4 * packets[0].shape[1] + LANES
    shapes = [((count, own_rows, across), BF16) for count in (2, 2, 1)] + [((3, own_rows, across), F32)]
    shapes.append(((packets[0].shape[1], JUMP * columns), BF16))

    def body(*refs):
        project_body(kv_size, own_rows, columns, *refs)

    scratch = [pltpu.VMEM((len(AHEAD) * own_rows, across), F32)]
    return kernel(body, [], [own_rows_wide, small_weights, *packets], shapes, scratch)


def combine_body(wide, kept_ref, up_ref, down_ref, across_ref, carried_ref, ahead_ref, behind_ref):
    del carried_ref
    for at, pieces, out_ref in ((1, (up_ref[1], across_ref[0]), ahead_ref), (2, (down_ref[1],), behind_ref)):
        big = kept_ref[at][:, :wide]
        small = kept_ref[at][:, wide:]
        for piece in pieces:
            more_big, more_small = joined(piece, wide)
            big = big + more_big
            small = small + more_small
        big, little = split(jnp.concatenate([big, small], axis=1), wide)
        out_ref[:, :wide] = big
        out_ref[:, wide:] = little


def combine(kept, up, down, across, carried):
    wide = kept.shape[2] - LANES

    def body(*refs):
        combine_body(wide, *refs)

    shapes = [(kept.shape[1:], BF16)] * 2
    return kernel(body, [], [kept, up, down, across, carried], shapes)


def deliver_body(rows_ref, weight_ref, out_ref):
    out_ref[...] = jnp.dot(rows_ref[...], weight_ref[...], preferred_element_type=F32).astype(BF16)


def deliver(rows, weight):
    (partial,) = kernel(deliver_body, [], [rows, weight], [((rows.shape[0], weight.shape[1]), BF16)])
    return partial


def reduce_body(terms_ref, *out_refs):
    columns = out_refs[0].shape[1]
    for at, out_ref in enumerate(out_refs):
        total = terms_ref[0, :, at * columns : (at + 1) * columns].astype(F32)
        for member in range(1, terms_ref.shape[0]):
            total = total + terms_ref[member, :, at * columns : (at + 1) * columns].astype(F32)
        out_ref[...] = total.astype(BF16)


def reduce_terms(terms):
    _, rows, wide = terms.shape
    return kernel(reduce_body, [], [terms], [((rows, wide // JUMP), BF16)] * JUMP)


def spread_body(*refs):
    out_ref = refs[-1]
    for at, piece_ref in enumerate(refs[:-1]):
        for member in range(out_ref.shape[0]):
            out_ref[member, at] = piece_ref[...]


def spread(pieces, copies):
    (out,) = kernel(spread_body, [], pieces, [((copies, len(pieces), *pieces[0].shape), BF16)])
    return out


def settle_body(blocks_ref, out_ref):
    shard_kv = lax.axis_index("kv")
    kv_size = blocks_ref.shape[0]
    for n in range(kv_size):
        owner = (shard_kv + n % JUMP + JUMP - WINDOW[-1]) % JUMP + n // JUMP * JUMP
        out_ref[owner] = blocks_ref[n]


def settle(blocks):
    (out,) = kernel(settle_body, [], [blocks], [(blocks.shape, BF16)], out_near=False)
    return out


def propose_body(
    span_size, total_heads, model_width, rate_ref, gain_ref, kept_ref, up_ref, down_ref, ahead_ref, behind_ref, state_ref, out_ref
):
    rows = kept_ref.shape[1]
    seq_count, heads_here, depth = state_ref.shape[0], state_ref.shape[1], state_ref.shape[2]
    wide = heads_here * depth

    def total(at, size):
        summed = kept_ref[0, :, at : at + size]
        for piece in (up_ref[0], down_ref[0], ahead_ref[...], behind_ref[...]):
            summed = summed + piece[:, at : at + size].astype(F32)
        return summed

    small = total(4 * wide, LANES)
    small = small + pltpu.roll(small, HALF, 1)
    lane = lax.broadcasted_iota(jnp.int32, small.shape, 1)

    def column(at):
        return jnp.sum(jnp.where(lane == at, small, F32(0.0)), axis=1, keepdims=True)

    inverse = lax.rsqrt(column(HALF - 1) / model_width + EPS)
    row = lax.broadcasted_iota(jnp.int32, (rows, 1), 0)
    place = row % span_size
    out_gain = gain_ref[...].astype(F32)

    def back(values, by):
        moved = pltpu.roll(values, by, 0)
        return jnp.where(place >= by, moved, F32(0.0))

    def dots(left, right):
        return jnp.sum(left * right, axis=1, keepdims=True)

    def unit(vectors):
        return vectors * lax.rsqrt(dots(vectors, vectors) + EPS)

    def over_lanes(values):
        return jnp.broadcast_to(values, (rows, depth))

    for head in range(heads_here):
        first = head * depth
        queries = unit(total(first, depth) * inverse) * F32(depth ** (-0.5))
        keys = unit(total(wide + first, depth) * inverse)
        values = total(2 * wide + first, depth) * inverse
        gate = total(3 * wide + first, depth) * inverse
        head_at = lax.axis_index("tp") * heads_here + head
        beta = over_lanes(jax.nn.sigmoid(column(head_at) * inverse))
        logit = over_lanes(column(total_heads + head_at) * inverse)
        softplus = jnp.maximum(logit, F32(0.0)) + jnp.log1p(jnp.exp(-jnp.abs(logit)))
        log_decay = -rate_ref[head] * softplus
        cumulative = log_decay
        for by in range(1, span_size):
            cumulative = cumulative + back(log_decay, by)
        grown = jnp.exp(cumulative)
        moved_keys = [keys] + [back(keys, by) for by in range(1, span_size)]
        within = [None] + [
            jnp.where(place >= by, jnp.exp(jnp.where(place >= by, cumulative - back(cumulative, by), F32(0.0))), F32(0.0))
            for by in range(1, span_size)
        ]
        lower = [None] + [beta * dots(keys, moved_keys[by]) * within[by] for by in range(1, span_size)]
        pushed = beta * values
        weighted = beta * grown * keys
        for step in range(1, span_size):
            at_step = place == step
            push_less = jnp.zeros_like(pushed)
            weight_less = jnp.zeros_like(weighted)
            for by in range(1, step + 1):
                push_less = push_less + lower[by] * back(pushed, by)
                weight_less = weight_less + lower[by] * back(weighted, by)
            pushed = pushed - jnp.where(at_step, push_less, F32(0.0))
            weighted = weighted - jnp.where(at_step, weight_less, F32(0.0))
        left = jnp.concatenate([weighted, queries * grown], axis=0)
        sequence = lax.broadcasted_iota(jnp.int32, (2 * rows, 1), 0) % rows // span_size
        read = jnp.zeros((2 * rows, depth), F32)
        for seq in range(seq_count):
            term = jnp.dot(left, state_ref[seq, head], precision=lax.Precision.HIGHEST, preferred_element_type=F32)
            read = jnp.where(sequence == seq, term, read)
        corrections = pushed - read[:rows]
        outputs = read[rows:] + dots(queries, keys) * corrections
        for by in range(1, span_size):
            outputs = outputs + dots(queries, moved_keys[by]) * within[by] * back(corrections, by)
        scale = lax.rsqrt(dots(outputs, outputs) / depth + EPS)
        finished = (outputs * scale * out_gain * (gate * jax.nn.sigmoid(gate))).astype(BF16)
        for copy in range(out_ref.shape[0] // rows):
            out_ref[copy * rows : (copy + 1) * rows, first : first + depth] = finished


def propose(decay_rate, out_gain, terms, carried, span_size, total_heads, model_width, copies):
    def body(*refs):
        propose_body(span_size, total_heads, model_width, *refs)

    wide = carried.shape[1] * carried.shape[2]
    shape = (copies * terms[0].shape[1], wide)
    operands = [out_gain.reshape(1, -1), *terms, carried]
    (hidden,) = kernel(body, [decay_rate], operands, [(shape, BF16)])
    return hidden


def shards(
    tokens,
    norm_gain,
    w_query,
    w_key,
    w_value,
    w_gate,
    w_beta,
    w_decay,
    decay_rate,
    out_gain,
    w_out,
    state,
    prev_keys,
    prev_values,
    prev_beta,
    prev_logdecay,
    accepted,
    kv_size,
    tp_size,
):
    seq_count = state.shape[0]
    span_size = prev_keys.shape[1]
    own_rows = seq_count * span_size
    model_width, total_heads = w_beta.shape
    weights = [w_query, w_key, w_value, w_gate]
    to_next, to_previous, own_rows_wide = pack(tokens, norm_gain[None, :], weights, w_out, kv_size, own_rows)
    before = shift(to_next, kv_size, 1)
    after = shift(to_previous, kv_size, -1)
    after2 = shift(after[: to_next.shape[0]], kv_size, -1)

    beta = prev_beta.reshape(-1)
    logdecay = prev_logdecay.reshape(-1)
    carried = replay(state, prev_keys, prev_values, beta, logdecay, accepted)
    small_weights = jnp.concatenate([w_beta.T, w_decay.T], axis=0)
    packets = (to_next, before, after, after2)
    up, down, across, kept, w_out_near = project(own_rows_wide, small_weights, packets, kv_size, own_rows)
    across = shift(across, kv_size, 2 * JUMP)
    up = shift(up, kv_size, JUMP)
    down = shift(down, kv_size, -JUMP)
    ahead, behind = combine(kept, up, down, across, carried)
    ahead = shift(ahead, kv_size, 2 * JUMP)
    behind = shift(behind, kv_size, -2 * JUMP)
    terms = (kept, up, down, ahead, behind)
    members = kv_size // JUMP
    hidden = propose(decay_rate, out_gain, terms, carried, span_size, total_heads, model_width, members)
    groups = [list(range(first, kv_size, JUMP)) for first in range(JUMP)]
    rows_all = lax.all_to_all(hidden, "kv", 0, 0, tiled=True, axis_index_groups=groups)
    partial = deliver(rows_all, w_out_near)
    exchanged = lax.all_to_all(partial, "tp", 0, 0, tiled=True)
    finished = reduce_terms(exchanged.reshape(tp_size, own_rows, -1))
    landed = [
        piece if offset == 0 else shift(piece, kv_size, offset) for offset, piece in zip(WINDOW, finished)
    ][::-1]
    copies = spread(landed, tp_size).reshape(kv_size * own_rows, -1)
    mixed = lax.all_to_all(copies, "tp", 0, 0, tiled=True)
    mixed = settle(mixed.reshape(kv_size, own_rows, -1)).reshape(kv_size * own_rows, -1)
    return (mixed, carried)


def solution(mesh):
    in_specs = (
        P("grp", "kv"),
        P("kv"),
        P("kv", "tp"),
        P("kv", "tp"),
        P("kv", "tp"),
        P("kv", "tp"),
        P(),
        P(),
        P("tp"),
        P(),
        P("tp", "kv"),
        P(("grp", "kv"), "tp", None, None),
        P(("grp", "kv"), None, "tp", None),
        P(("grp", "kv"), None, "tp", None),
        P(("grp", "kv"), None, "tp"),
        P(("grp", "kv"), None, "tp"),
        P(("grp", "kv")),
    )
    out_specs = (P("grp", "kv"), P(("grp", "kv"), "tp", None, None))

    def per_device(*arguments):
        return shards(*arguments, kv_size=mesh.shape["kv"], tp_size=mesh.shape["tp"])

    return jax.shard_map(per_device, mesh=mesh, in_specs=in_specs, out_specs=out_specs, check_vma=False)
```

```python
import jax
import jax.numpy as jnp
from jax import lax
from jax.experimental import pallas as pl
from jax.experimental.pallas import tpu as pltpu
from jax.sharding import PartitionSpec as P


EPS = 1e-06
WINDOW = (-1, 0, 1, 2)
JUMP = len(WINDOW)
NEAR_OUT = 8
AHEAD = (0, JUMP, -JUMP, 2 * JUMP, -2 * JUMP, 3 * JUMP, -3 * JUMP, 4 * JUMP)
LANES = 128
HALF = LANES // 2
F32 = jnp.float32
BF16 = jnp.bfloat16


def near_memory(array):
    return pltpu.with_memory_space_constraint(array, pltpu.MemorySpace.VMEM)


def kernel(body, scalars, arrays, shapes, scratch=(), in_near=True, out_near=True):
    smem = pl.BlockSpec(memory_space=pltpu.SMEM)
    vmem = pl.BlockSpec(memory_space=pltpu.VMEM)
    kind = pltpu.VMEM if out_near else jax.ShapeDtypeStruct
    return pl.pallas_call(
        body,
        in_specs=[smem] * len(scalars) + [vmem] * len(arrays),
        out_specs=[vmem] * len(shapes),
        out_shape=[kind(shape, dtype) for shape, dtype in shapes],
        scratch_shapes=list(scratch),
    )(*scalars, *[near_memory(array) if in_near else array for array in arrays])


def shift(table, axis_size, by):
    return lax.ppermute(table, "kv", [(i, (i + by) % axis_size) for i in range(axis_size)])


def replay_body(beta_ref, logdecay_ref, accepted_ref, keys_ref, values_ref, state_ref, out_ref, rows_ref):
    seq_count, span_size, heads_here, depth = keys_ref.shape
    rows_ref[...] = jnp.zeros(rows_ref.shape, F32)

    def one(seq, carry):
        for position in range(span_size):
            first = position * heads_here
            keys = keys_ref[seq, position].astype(F32)
            keys = keys * lax.rsqrt(jnp.sum(keys * keys, axis=-1, keepdims=True) + EPS)
            rows_ref[first : first + heads_here, :] = keys
        key_columns = jnp.transpose(rows_ref[...])
        for head in range(heads_here):
            state = state_ref[seq, head]
            for position in range(span_size):
                row = position * heads_here + head
                spot = seq * span_size * heads_here + row
                active = accepted_ref[seq] > position
                logdecay = jnp.where(active, logdecay_ref[spot], F32(0.0))
                strength = jnp.where(active, beta_ref[spot], F32(0.0))
                column = jnp.broadcast_to(key_columns[:, row : row + 1], (depth, depth))
                state = jnp.exp(jnp.full((1, depth), logdecay, F32)) * state
                predicted = jnp.sum(column * state, axis=0, keepdims=True)
                value = values_ref[seq, position].astype(F32)[head : head + 1]
                state = state + column * (strength * (value - predicted))
            out_ref[seq, head] = state
        return carry

    lax.fori_loop(0, seq_count, one, 0)


def replay(state, prev_keys, prev_values, beta, logdecay, accepted):
    rows = -(-prev_keys.shape[1] * prev_keys.shape[2] // 8) * 8
    scratch = [pltpu.VMEM((rows, state.shape[-1]), F32)]
    scalars = [beta, logdecay, accepted]
    (carried,) = kernel(replay_body, scalars, [prev_keys, prev_values, state], [(state.shape, F32)], scratch)
    return carried


def rows_for(wide_ref, device, kv_size, own_rows):
    owners = [(device + ahead + 2 * kv_size) % kv_size for ahead in AHEAD]
    pieces = [wide_ref[pl.ds(pl.multiple_of(owner * own_rows, 8), own_rows), :] for owner in owners]
    return jnp.concatenate(pieces, axis=0)


def side_by_side(rows):
    half = rows.shape[0] // 2
    return jnp.concatenate([rows[:half], rows[half:]], axis=1).astype(BF16)


def layout(columns, own_rows):
    weights_at = 0
    gain_at = weights_at + 4 * columns
    rows_at = gain_at + 16
    return weights_at, gain_at, rows_at, len(AHEAD) * own_rows // 2


def pack_body(
    kv_size, own_rows, tokens_ref, gain_ref, wq_ref, wk_ref, wv_ref, wg_ref, next_ref, previous_ref, own_ref, wide_ref
):
    columns = gain_ref.shape[1]
    weights_at, gain_at, rows_at, half = layout(columns, own_rows)
    shard_kv = lax.axis_index("kv")
    wide_ref[...] = tokens_ref[...].astype(F32)
    own_ref[...] = rows_for(wide_ref, shard_kv, kv_size, own_rows)
    gain = jnp.concatenate([gain_ref[...]] * (wq_ref.shape[1] // columns), axis=1)
    gain = jnp.broadcast_to(gain, (16, wq_ref.shape[1]))
    for out_ref, stops in ((next_ref, (1,)), (previous_ref, (-2, -1))):
        for j, weight_ref in enumerate((wq_ref, wk_ref, wv_ref, wg_ref)):
            out_ref[weights_at + j * columns : weights_at + (j + 1) * columns, :] = weight_ref[...]
        out_ref[gain_at:rows_at, :] = gain
        for at, stop in enumerate(stops):
            rows = side_by_side(rows_for(wide_ref, shard_kv + stop, kv_size, own_rows))
            out_ref[rows_at + at * half : rows_at + (at + 1) * half, :] = rows


def pack(tokens, gain, weights, kv_size, own_rows):
    columns = tokens.shape[1]
    _, _, rows_at, half = layout(columns, own_rows)
    wide = weights[0].shape[1]

    def body(*refs):
        pack_body(kv_size, own_rows, *refs)

    shapes = [((rows_at + stops * half, wide), BF16) for stops in (1, 2)] + [((2 * half, columns), F32)]
    scratch = [pltpu.VMEM(tokens.shape, F32)]
    return kernel(body, [], [tokens, gain, *weights], shapes, scratch, in_near=False)


def split(values, wide):
    small = values[:, wide:]
    lane = lax.broadcasted_iota(jnp.int32, small.shape, 1)
    coarse = small.astype(BF16).astype(F32)
    rest = pltpu.roll(small - coarse, HALF, 1)
    return values[:, :wide].astype(BF16), jnp.where(lane < HALF, coarse, rest).astype(BF16)


def joined(terms, wide):
    small = terms[:, wide:].astype(F32)
    lane = lax.broadcasted_iota(jnp.int32, small.shape, 1)
    small = jnp.where(lane < HALF, small + pltpu.roll(small, HALF, 1), F32(0.0))
    return terms[:, :wide].astype(F32), small


def project_body(
    kv_size,
    own_rows,
    columns,
    own_rows_ref,
    small_ref,
    own_ref,
    before_ref,
    after_ref,
    after2_ref,
    up_ref,
    down_ref,
    across_ref,
    kept_ref,
    sums_ref,
):
    wide = own_ref.shape[1]
    weights_at, gain_at, rows_at, half = layout(columns, own_rows)
    shard_kv = lax.axis_index("kv")

    def taken(pay_ref, at):
        weights = [pay_ref[weights_at + j * columns : weights_at + (j + 1) * columns, :] for j in range(4)]
        gain = pay_ref[gain_at:rows_at, :columns].astype(F32)[:1]
        if at is None:
            return own_rows_ref[...], gain, weights
        both = pay_ref[rows_at + at * half : rows_at + (at + 1) * half, :].astype(F32)
        return jnp.concatenate([both[:, :columns], both[:, columns:]], axis=0), gain, weights

    parts = [taken(before_ref, 0), taken(own_ref, None), taken(after_ref, 1), taken(after2_ref, 0)]
    sums = [None] * 4
    small = None
    squares = None
    for at, (widened, gain, weights) in enumerate(parts):
        term = jnp.sum(widened * widened, axis=1, keepdims=True)
        squares = term if squares is None else squares + term
        scaled = (widened * gain).astype(BF16)
        for j in range(4):
            term = jnp.dot(scaled, weights[j], preferred_element_type=F32)
            sums[j] = term if sums[j] is None else sums[j] + term
        small_at = pl.multiple_of((shard_kv + WINDOW[at] + kv_size) % kv_size * columns, columns)
        term = lax.dot_general(
            scaled, small_ref[:, pl.ds(small_at, columns)], (((1,), (1,)), ((), ())), preferred_element_type=F32
        )
        small = term if small is None else small + term
    for j in range(4):
        sums_ref[:, j * wide : (j + 1) * wide] = sums[j]
    lane = lax.broadcasted_iota(jnp.int32, (small.shape[0], LANES), 1)
    sums_ref[:, 4 * wide :] = jnp.where(lane == HALF - 1, squares, F32(0.0))
    sums_ref[:, 4 * wide : 4 * wide + small.shape[1]] = small

    def block(ahead):
        start = AHEAD.index(ahead) * own_rows
        return sums_ref[start : start + own_rows, :]

    for out_ref, at, ahead in (
        (up_ref, 0, JUMP),
        (up_ref, 1, 3 * JUMP),
        (down_ref, 0, -JUMP),
        (down_ref, 1, -3 * JUMP),
        (across_ref, 0, 4 * JUMP),
    ):
        big, little = split(block(ahead), 4 * wide)
        out_ref[at, :, : 4 * wide] = big
        out_ref[at, :, 4 * wide :] = little
    for at, ahead in enumerate((0, 2 * JUMP, -2 * JUMP)):
        kept_ref[at] = block(ahead)


def project(own_rows_wide, small_weights, packets, kv_size, own_rows):
    columns = own_rows_wide.shape[1]
    across = 4 * packets[0].shape[1] + LANES
    shapes = [((count, own_rows, across), BF16) for count in (2, 2, 1)] + [((3, own_rows, across), F32)]

    def body(*refs):
        project_body(kv_size, own_rows, columns, *refs)

    scratch = [pltpu.VMEM((len(AHEAD) * own_rows, across), F32)]
    return kernel(body, [], [own_rows_wide, small_weights, *packets], shapes, scratch)


def combine_body(wide, kept_ref, up_ref, down_ref, across_ref, carried_ref, ahead_ref, behind_ref):
    del carried_ref
    for at, pieces, out_ref in ((1, (up_ref[1], across_ref[0]), ahead_ref), (2, (down_ref[1],), behind_ref)):
        big = kept_ref[at][:, :wide]
        small = kept_ref[at][:, wide:]
        for piece in pieces:
            more_big, more_small = joined(piece, wide)
            big = big + more_big
            small = small + more_small
        big, little = split(jnp.concatenate([big, small], axis=1), wide)
        out_ref[:, :wide] = big
        out_ref[:, wide:] = little


def combine(kept, up, down, across, carried):
    wide = kept.shape[2] - LANES

    def body(*refs):
        combine_body(wide, *refs)

    shapes = [(kept.shape[1:], BF16)] * 2
    return kernel(body, [], [kept, up, down, across, carried], shapes)


def deliver_near_body(kv_size, weight_ref, left_ref, three_ref, right_ref, out_ref):
    shard_kv = lax.axis_index("kv")
    own_rows = out_ref.shape[1]
    far_members = kv_size // NEAR_OUT
    pieces = [left_ref[0], left_ref[1], left_ref[2], three_ref[0], three_ref[1], three_ref[2], right_ref[0], right_ref[1]]
    for n, piece in enumerate(pieces):
        product = jnp.dot(piece, weight_ref[...], preferred_element_type=F32)
        for j in range(far_members):
            owner = (shard_kv + n - 4 + NEAR_OUT * (j - 2) + kv_size) % kv_size
            out_ref[owner] = product[j * own_rows : (j + 1) * own_rows].astype(BF16)


def deliver_near(w_out, left, three, right, kv_size, own_rows):
    def body(*refs):
        deliver_near_body(kv_size, *refs)

    shape = (kv_size, own_rows, w_out.shape[1])
    (partial,) = kernel(body, [], [w_out, left, three, right], [(shape, BF16)])
    return partial


def reduce_all_body(terms_ref, out_ref):
    total = terms_ref[0].astype(F32)
    for member in range(1, terms_ref.shape[0]):
        total = total + terms_ref[member].astype(F32)
    for member in range(terms_ref.shape[0]):
        out_ref[member] = total.astype(BF16)


def reduce_all(terms):
    (copies,) = kernel(reduce_all_body, [], [terms], [(terms.shape, BF16)])
    return copies


def stack_body(*refs):
    out_ref = refs[-1]
    for at, ref in enumerate(refs[:-1]):
        out_ref[at] = ref[...]


def stacked(pieces):
    (out,) = kernel(stack_body, [], pieces, [((len(pieces), *pieces[0].shape), BF16)])
    return out


def propose_body(
    span_size, total_heads, model_width, rate_ref, gain_ref, kept_ref, up_ref, down_ref, ahead_ref, behind_ref, state_ref, out_ref
):
    rows = kept_ref.shape[1]
    seq_count, heads_here, depth = state_ref.shape[0], state_ref.shape[1], state_ref.shape[2]
    wide = heads_here * depth

    def total(at, size):
        summed = kept_ref[0, :, at : at + size]
        for piece in (up_ref[0], down_ref[0], ahead_ref[...], behind_ref[...]):
            summed = summed + piece[:, at : at + size].astype(F32)
        return summed

    small = total(4 * wide, LANES)
    small = small + pltpu.roll(small, HALF, 1)
    lane = lax.broadcasted_iota(jnp.int32, small.shape, 1)

    def column(at):
        return jnp.sum(jnp.where(lane == at, small, F32(0.0)), axis=1, keepdims=True)

    inverse = lax.rsqrt(column(HALF - 1) / model_width + EPS)
    row = lax.broadcasted_iota(jnp.int32, (rows, 1), 0)
    place = row % span_size
    out_gain = gain_ref[...].astype(F32)

    def back(values, by):
        moved = pltpu.roll(values, by, 0)
        return jnp.where(place >= by, moved, F32(0.0))

    def dots(left, right):
        return jnp.sum(left * right, axis=1, keepdims=True)

    def unit(vectors):
        return vectors * lax.rsqrt(dots(vectors, vectors) + EPS)

    def over_lanes(values):
        return jnp.broadcast_to(values, (rows, depth))

    for head in range(heads_here):
        first = head * depth
        queries = unit(total(first, depth) * inverse) * F32(depth ** (-0.5))
        keys = unit(total(wide + first, depth) * inverse)
        values = total(2 * wide + first, depth) * inverse
        gate = total(3 * wide + first, depth) * inverse
        head_at = lax.axis_index("tp") * heads_here + head
        beta = over_lanes(jax.nn.sigmoid(column(head_at) * inverse))
        logit = over_lanes(column(total_heads + head_at) * inverse)
        softplus = jnp.maximum(logit, F32(0.0)) + jnp.log1p(jnp.exp(-jnp.abs(logit)))
        log_decay = -rate_ref[head] * softplus
        cumulative = log_decay
        for by in range(1, span_size):
            cumulative = cumulative + back(log_decay, by)
        grown = jnp.exp(cumulative)
        moved_keys = [keys] + [back(keys, by) for by in range(1, span_size)]
        within = [None] + [
            jnp.where(place >= by, jnp.exp(jnp.where(place >= by, cumulative - back(cumulative, by), F32(0.0))), F32(0.0))
            for by in range(1, span_size)
        ]
        lower = [None] + [beta * dots(keys, moved_keys[by]) * within[by] for by in range(1, span_size)]
        pushed = beta * values
        weighted = beta * grown * keys
        for step in range(1, span_size):
            at_step = place == step
            push_less = jnp.zeros_like(pushed)
            weight_less = jnp.zeros_like(weighted)
            for by in range(1, step + 1):
                push_less = push_less + lower[by] * back(pushed, by)
                weight_less = weight_less + lower[by] * back(weighted, by)
            pushed = pushed - jnp.where(at_step, push_less, F32(0.0))
            weighted = weighted - jnp.where(at_step, weight_less, F32(0.0))
        left = jnp.concatenate([weighted, queries * grown], axis=0)
        sequence = lax.broadcasted_iota(jnp.int32, (2 * rows, 1), 0) % rows // span_size
        read = jnp.zeros((2 * rows, depth), F32)
        for seq in range(seq_count):
            term = jnp.dot(left, state_ref[seq, head], precision=lax.Precision.HIGHEST, preferred_element_type=F32)
            read = jnp.where(sequence == seq, term, read)
        corrections = pushed - read[:rows]
        outputs = read[rows:] + dots(queries, keys) * corrections
        for by in range(1, span_size):
            outputs = outputs + dots(queries, moved_keys[by]) * within[by] * back(corrections, by)
        scale = lax.rsqrt(dots(outputs, outputs) / depth + EPS)
        finished = (outputs * scale * out_gain * (gate * jax.nn.sigmoid(gate))).astype(BF16)
        out_ref[:, first : first + depth] = finished


def propose(decay_rate, out_gain, terms, carried, span_size, total_heads, model_width):
    def body(*refs):
        propose_body(span_size, total_heads, model_width, *refs)

    wide = carried.shape[1] * carried.shape[2]
    shape = (terms[0].shape[1], wide)
    operands = [out_gain.reshape(1, -1), *terms, carried]
    (hidden,) = kernel(body, [decay_rate], operands, [(shape, BF16)])
    return hidden


def shards(
    tokens,
    norm_gain,
    w_query,
    w_key,
    w_value,
    w_gate,
    w_beta,
    w_decay,
    decay_rate,
    out_gain,
    w_out,
    state,
    prev_keys,
    prev_values,
    prev_beta,
    prev_logdecay,
    accepted,
    kv_size,
    tp_size,
):
    seq_count = state.shape[0]
    span_size = prev_keys.shape[1]
    own_rows = seq_count * span_size
    model_width, total_heads = w_beta.shape
    weights = [w_query, w_key, w_value, w_gate]
    to_next, to_previous, own_rows_wide = pack(tokens, norm_gain[None, :], weights, kv_size, own_rows)
    before = shift(to_next, kv_size, 1)
    after = shift(to_previous, kv_size, -1)
    after2 = shift(after[: to_next.shape[0]], kv_size, -1)

    beta = prev_beta.reshape(-1)
    logdecay = prev_logdecay.reshape(-1)
    carried = replay(state, prev_keys, prev_values, beta, logdecay, accepted)
    small_weights = jnp.concatenate([w_beta.T, w_decay.T], axis=0)
    packets = (to_next, before, after, after2)
    up, down, across, kept = project(own_rows_wide, small_weights, packets, kv_size, own_rows)
    across = shift(across, kv_size, 2 * JUMP)
    up = shift(up, kv_size, JUMP)
    down = shift(down, kv_size, -JUMP)
    ahead, behind = combine(kept, up, down, across, carried)
    ahead = shift(ahead, kv_size, 2 * JUMP)
    behind = shift(behind, kv_size, -2 * JUMP)
    terms = (kept, up, down, ahead, behind)
    hidden = propose(decay_rate, out_gain, terms, carried, span_size, total_heads, model_width)
    below = shift(hidden, kv_size, NEAR_OUT)
    above = shift(hidden, kv_size, -NEAR_OUT)
    opposite = shift(below, kv_size, NEAR_OUT)
    block = stacked([opposite, below, hidden, above]).reshape(4 * own_rows, -1)
    left = shift(block, kv_size, 1)
    right = shift(block, kv_size, -1)
    three = stacked([left, block, right])
    near_left = shift(three, kv_size, 3)
    near_right = shift(three[:2], kv_size, -3)
    partial = deliver_near(w_out, near_left, three, near_right, kv_size, own_rows)
    partial = partial.reshape(kv_size * own_rows, -1)
    exchanged = lax.all_to_all(partial, "tp", 0, 0, tiled=True)
    copies = reduce_all(exchanged.reshape(tp_size, -1, exchanged.shape[1]))
    mixed = lax.all_to_all(copies.reshape(exchanged.shape), "tp", 0, 0, tiled=True)
    return (mixed, carried)


def solution(mesh):
    in_specs = (
        P("grp", "kv"),
        P("kv"),
        P("kv", "tp"),
        P("kv", "tp"),
        P("kv", "tp"),
        P("kv", "tp"),
        P(),
        P(),
        P("tp"),
        P(),
        P("tp", "kv"),
        P(("grp", "kv"), "tp", None, None),
        P(("grp", "kv"), None, "tp", None),
        P(("grp", "kv"), None, "tp", None),
        P(("grp", "kv"), None, "tp"),
        P(("grp", "kv"), None, "tp"),
        P(("grp", "kv")),
    )
    out_specs = (P("grp", "kv"), P(("grp", "kv"), "tp", None, None))

    def per_device(*arguments):
        return shards(*arguments, kv_size=mesh.shape["kv"], tp_size=mesh.shape["tp"])

    return jax.shard_map(per_device, mesh=mesh, in_specs=in_specs, out_specs=out_specs, check_vma=False)
```

```python
import jax
import jax.numpy as jnp
from jax import lax
from jax.experimental import pallas as pl
from jax.experimental.pallas import tpu as pltpu
from jax.sharding import PartitionSpec as P


EPS = 1e-06
WINDOW = (-1, 0, 1, 2)
JUMP = len(WINDOW)
AHEAD = (0, JUMP, -JUMP, 2 * JUMP, -2 * JUMP, 3 * JUMP, -3 * JUMP, 4 * JUMP)
LANES = 128
HALF = LANES // 2
F32 = jnp.float32
BF16 = jnp.bfloat16


def near_memory(array):
    return pltpu.with_memory_space_constraint(array, pltpu.MemorySpace.VMEM)


def kernel(body, scalars, arrays, shapes, scratch=(), in_near=True, out_near=True):
    smem = pl.BlockSpec(memory_space=pltpu.SMEM)
    vmem = pl.BlockSpec(memory_space=pltpu.VMEM)
    kind = pltpu.VMEM if out_near else jax.ShapeDtypeStruct
    return pl.pallas_call(
        body,
        in_specs=[smem] * len(scalars) + [vmem] * len(arrays),
        out_specs=[vmem] * len(shapes),
        out_shape=[kind(shape, dtype) for shape, dtype in shapes],
        scratch_shapes=list(scratch),
    )(*scalars, *[near_memory(array) if in_near else array for array in arrays])


def shift(table, axis_size, by):
    return lax.ppermute(table, "kv", [(i, (i + by) % axis_size) for i in range(axis_size)])


def replay_body(beta_ref, logdecay_ref, accepted_ref, keys_ref, values_ref, state_ref, out_ref, rows_ref):
    seq_count, span_size, heads_here, depth = keys_ref.shape
    rows_ref[...] = jnp.zeros(rows_ref.shape, F32)

    def one(seq, carry):
        for position in range(span_size):
            first = position * heads_here
            keys = keys_ref[seq, position].astype(F32)
            keys = keys * lax.rsqrt(jnp.sum(keys * keys, axis=-1, keepdims=True) + EPS)
            rows_ref[first : first + heads_here, :] = keys
        key_columns = jnp.transpose(rows_ref[...])
        for head in range(heads_here):
            state = state_ref[seq, head]
            for position in range(span_size):
                row = position * heads_here + head
                spot = seq * span_size * heads_here + row
                active = accepted_ref[seq] > position
                logdecay = jnp.where(active, logdecay_ref[spot], F32(0.0))
                strength = jnp.where(active, beta_ref[spot], F32(0.0))
                column = jnp.broadcast_to(key_columns[:, row : row + 1], (depth, depth))
                state = jnp.exp(jnp.full((1, depth), logdecay, F32)) * state
                predicted = jnp.sum(column * state, axis=0, keepdims=True)
                value = values_ref[seq, position].astype(F32)[head : head + 1]
                state = state + column * (strength * (value - predicted))
            out_ref[seq, head] = state
        return carry

    lax.fori_loop(0, seq_count, one, 0)


def replay(state, prev_keys, prev_values, beta, logdecay, accepted):
    rows = -(-prev_keys.shape[1] * prev_keys.shape[2] // 8) * 8
    scratch = [pltpu.VMEM((rows, state.shape[-1]), F32)]
    scalars = [beta, logdecay, accepted]
    (carried,) = kernel(replay_body, scalars, [prev_keys, prev_values, state], [(state.shape, F32)], scratch)
    return carried


def rows_for(wide_ref, device, kv_size, own_rows):
    owners = [(device + ahead + 2 * kv_size) % kv_size for ahead in AHEAD]
    pieces = [wide_ref[pl.ds(pl.multiple_of(owner * own_rows, 8), own_rows), :] for owner in owners]
    return jnp.concatenate(pieces, axis=0)


def side_by_side(rows):
    half = rows.shape[0] // 2
    return jnp.concatenate([rows[:half], rows[half:]], axis=1).astype(BF16)


def layout(columns, own_rows):
    weights_at = columns
    gain_at = weights_at + 4 * columns
    rows_at = gain_at + 16
    return weights_at, gain_at, rows_at, len(AHEAD) * own_rows // 2


def pack_body(
    kv_size, own_rows, tokens_ref, gain_ref, wq_ref, wk_ref, wv_ref, wg_ref, wo_ref, next_ref, previous_ref, own_ref, wide_ref
):
    columns = gain_ref.shape[1]
    weights_at, gain_at, rows_at, half = layout(columns, own_rows)
    shard_kv = lax.axis_index("kv")
    wide_ref[...] = tokens_ref[...].astype(F32)
    own_ref[...] = rows_for(wide_ref, shard_kv, kv_size, own_rows)
    gain = jnp.concatenate([gain_ref[...]] * (wq_ref.shape[1] // columns), axis=1)
    gain = jnp.broadcast_to(gain, (16, wq_ref.shape[1]))
    for out_ref, stops in ((next_ref, (1,)), (previous_ref, (-2, -1))):
        out_ref[:columns, :columns] = wo_ref[:columns, :]
        out_ref[:columns, columns:] = wo_ref[columns:, :]
        for j, weight_ref in enumerate((wq_ref, wk_ref, wv_ref, wg_ref)):
            out_ref[weights_at + j * columns : weights_at + (j + 1) * columns, :] = weight_ref[...]
        out_ref[gain_at:rows_at, :] = gain
        for at, stop in enumerate(stops):
            rows = side_by_side(rows_for(wide_ref, shard_kv + stop, kv_size, own_rows))
            out_ref[rows_at + at * half : rows_at + (at + 1) * half, :] = rows


def pack(tokens, gain, weights, w_out, kv_size, own_rows):
    columns = tokens.shape[1]
    _, _, rows_at, half = layout(columns, own_rows)
    wide = weights[0].shape[1]

    def body(*refs):
        pack_body(kv_size, own_rows, *refs)

    shapes = [((rows_at + stops * half, wide), BF16) for stops in (1, 2)] + [((2 * half, columns), F32)]
    scratch = [pltpu.VMEM(tokens.shape, F32)]
    return kernel(body, [], [tokens, gain, *weights, w_out], shapes, scratch, in_near=False)


def split(values, wide):
    small = values[:, wide:]
    lane = lax.broadcasted_iota(jnp.int32, small.shape, 1)
    coarse = small.astype(BF16).astype(F32)
    rest = pltpu.roll(small - coarse, HALF, 1)
    return values[:, :wide].astype(BF16), jnp.where(lane < HALF, coarse, rest).astype(BF16)


def joined(terms, wide):
    small = terms[:, wide:].astype(F32)
    lane = lax.broadcasted_iota(jnp.int32, small.shape, 1)
    small = jnp.where(lane < HALF, small + pltpu.roll(small, HALF, 1), F32(0.0))
    return terms[:, :wide].astype(F32), small


def project_body(
    kv_size,
    own_rows,
    columns,
    own_rows_ref,
    small_ref,
    own_ref,
    before_ref,
    after_ref,
    after2_ref,
    up_ref,
    down_ref,
    across_ref,
    kept_ref,
    w_out_ref,
    sums_ref,
):
    for at, packet_ref in enumerate((before_ref, own_ref, after_ref, after2_ref)):
        for part in range(w_out_ref.shape[0] // columns):
            piece = packet_ref[:columns, part * columns : (part + 1) * columns]
            w_out_ref[part * columns : (part + 1) * columns, at * columns : (at + 1) * columns] = piece
    wide = own_ref.shape[1]
    weights_at, gain_at, rows_at, half = layout(columns, own_rows)
    shard_kv = lax.axis_index("kv")

    def taken(pay_ref, at):
        weights = [pay_ref[weights_at + j * columns : weights_at + (j + 1) * columns, :] for j in range(4)]
        gain = pay_ref[gain_at:rows_at, :columns].astype(F32)[:1]
        if at is None:
            return own_rows_ref[...], gain, weights
        both = pay_ref[rows_at + at * half : rows_at + (at + 1) * half, :].astype(F32)
        return jnp.concatenate([both[:, :columns], both[:, columns:]], axis=0), gain, weights

    parts = [taken(before_ref, 0), taken(own_ref, None), taken(after_ref, 1), taken(after2_ref, 0)]
    sums = [None] * 4
    small = None
    squares = None
    for at, (widened, gain, weights) in enumerate(parts):
        term = jnp.sum(widened * widened, axis=1, keepdims=True)
        squares = term if squares is None else squares + term
        scaled = (widened * gain).astype(BF16)
        for j in range(4):
            term = jnp.dot(scaled, weights[j], preferred_element_type=F32)
            sums[j] = term if sums[j] is None else sums[j] + term
        small_at = pl.multiple_of((shard_kv + WINDOW[at] + kv_size) % kv_size * columns, columns)
        term = lax.dot_general(
            scaled, small_ref[:, pl.ds(small_at, columns)], (((1,), (1,)), ((), ())), preferred_element_type=F32
        )
        small = term if small is None else small + term
    for j in range(4):
        sums_ref[:, j * wide : (j + 1) * wide] = sums[j]
    lane = lax.broadcasted_iota(jnp.int32, (small.shape[0], LANES), 1)
    sums_ref[:, 4 * wide :] = jnp.where(lane == HALF - 1, squares, F32(0.0))
    sums_ref[:, 4 * wide : 4 * wide + small.shape[1]] = small

    def block(ahead):
        start = AHEAD.index(ahead) * own_rows
        return sums_ref[start : start + own_rows, :]

    for out_ref, at, ahead in (
        (up_ref, 0, JUMP),
        (up_ref, 1, 3 * JUMP),
        (down_ref, 0, -JUMP),
        (down_ref, 1, -3 * JUMP),
        (across_ref, 0, 4 * JUMP),
    ):
        big, little = split(block(ahead), 4 * wide)
        out_ref[at, :, : 4 * wide] = big
        out_ref[at, :, 4 * wide :] = little
    for at, ahead in enumerate((0, 2 * JUMP, -2 * JUMP)):
        kept_ref[at] = block(ahead)


def project(own_rows_wide, small_weights, packets, kv_size, own_rows):
    columns = own_rows_wide.shape[1]
    across = 4 * packets[0].shape[1] + LANES
    shapes = [((count, own_rows, across), BF16) for count in (2, 2, 1)] + [((3, own_rows, across), F32)]
    shapes.append(((packets[0].shape[1], JUMP * columns), BF16))

    def body(*refs):
        project_body(kv_size, own_rows, columns, *refs)

    scratch = [pltpu.VMEM((len(AHEAD) * own_rows, across), F32)]
    return kernel(body, [], [own_rows_wide, small_weights, *packets], shapes, scratch)


def combine_body(wide, kept_ref, up_ref, down_ref, across_ref, carried_ref, ahead_ref, behind_ref):
    del carried_ref
    for at, pieces, out_ref in ((1, (up_ref[1], across_ref[0]), ahead_ref), (2, (down_ref[1],), behind_ref)):
        big = kept_ref[at][:, :wide]
        small = kept_ref[at][:, wide:]
        for piece in pieces:
            more_big, more_small = joined(piece, wide)
            big = big + more_big
            small = small + more_small
        big, little = split(jnp.concatenate([big, small], axis=1), wide)
        out_ref[:, :wide] = big
        out_ref[:, wide:] = little


def combine(kept, up, down, across, carried):
    wide = kept.shape[2] - LANES

    def body(*refs):
        combine_body(wide, *refs)

    shapes = [(kept.shape[1:], BF16)] * 2
    return kernel(body, [], [kept, up, down, across, carried], shapes)


def deliver_body(*refs):
    *row_refs, weight_ref, out_ref = refs
    rows = jnp.concatenate([ref[...].astype(F32) for ref in row_refs], axis=0).astype(BF16)
    out_ref[...] = jnp.dot(rows, weight_ref[...], preferred_element_type=F32).astype(BF16)


def deliver(pieces, weight):
    shape = (sum(piece.shape[0] for piece in pieces), weight.shape[1])
    (partial,) = kernel(deliver_body, [], [*pieces, weight], [(shape, BF16)])
    return partial


def reduce_body(terms_ref, *out_refs):
    columns = out_refs[0].shape[1]
    for at, out_ref in enumerate(out_refs):
        total = terms_ref[0, :, at * columns : (at + 1) * columns].astype(F32)
        for member in range(1, terms_ref.shape[0]):
            total = total + terms_ref[member, :, at * columns : (at + 1) * columns].astype(F32)
        out_ref[...] = total.astype(BF16)


def reduce_terms(terms):
    _, rows, wide = terms.shape
    return kernel(reduce_body, [], [terms], [((rows, wide // JUMP), BF16)] * JUMP)


def spread_body(*refs):
    out_ref = refs[-1]
    for at, piece_ref in enumerate(refs[:-1]):
        for member in range(out_ref.shape[0]):
            out_ref[member, at] = piece_ref[...]


def spread(pieces, copies):
    (out,) = kernel(spread_body, [], pieces, [((copies, len(pieces), *pieces[0].shape), BF16)])
    return out


def settle_body(blocks_ref, out_ref):
    shard_kv = lax.axis_index("kv")
    kv_size = blocks_ref.shape[0]
    for n in range(kv_size):
        owner = (shard_kv + n + kv_size - WINDOW[-1] - kv_size // 2) % kv_size
        out_ref[owner] = blocks_ref[n]


def settle(blocks):
    (out,) = kernel(settle_body, [], [blocks], [(blocks.shape, BF16)], out_near=False)
    return out


def propose_body(
    span_size, total_heads, model_width, rate_ref, gain_ref, kept_ref, up_ref, down_ref, ahead_ref, behind_ref, state_ref, out_ref
):
    rows = kept_ref.shape[1]
    seq_count, heads_here, depth = state_ref.shape[0], state_ref.shape[1], state_ref.shape[2]
    wide = heads_here * depth

    def total(at, size):
        summed = kept_ref[0, :, at : at + size]
        for piece in (up_ref[0], down_ref[0], ahead_ref[...], behind_ref[...]):
            summed = summed + piece[:, at : at + size].astype(F32)
        return summed

    small = total(4 * wide, LANES)
    small = small + pltpu.roll(small, HALF, 1)
    lane = lax.broadcasted_iota(jnp.int32, small.shape, 1)

    def column(at):
        return jnp.sum(jnp.where(lane == at, small, F32(0.0)), axis=1, keepdims=True)

    inverse = lax.rsqrt(column(HALF - 1) / model_width + EPS)
    row = lax.broadcasted_iota(jnp.int32, (rows, 1), 0)
    place = row % span_size
    out_gain = gain_ref[...].astype(F32)

    def back(values, by):
        moved = pltpu.roll(values, by, 0)
        return jnp.where(place >= by, moved, F32(0.0))

    def dots(left, right):
        return jnp.sum(left * right, axis=1, keepdims=True)

    def unit(vectors):
        return vectors * lax.rsqrt(dots(vectors, vectors) + EPS)

    def over_lanes(values):
        return jnp.broadcast_to(values, (rows, depth))

    for head in range(heads_here):
        first = head * depth
        queries = unit(total(first, depth) * inverse) * F32(depth ** (-0.5))
        keys = unit(total(wide + first, depth) * inverse)
        values = total(2 * wide + first, depth) * inverse
        gate = total(3 * wide + first, depth) * inverse
        head_at = lax.axis_index("tp") * heads_here + head
        beta = over_lanes(jax.nn.sigmoid(column(head_at) * inverse))
        logit = over_lanes(column(total_heads + head_at) * inverse)
        softplus = jnp.maximum(logit, F32(0.0)) + jnp.log1p(jnp.exp(-jnp.abs(logit)))
        log_decay = -rate_ref[head] * softplus
        cumulative = log_decay
        for by in range(1, span_size):
            cumulative = cumulative + back(log_decay, by)
        grown = jnp.exp(cumulative)
        moved_keys = [keys] + [back(keys, by) for by in range(1, span_size)]
        within = [None] + [
            jnp.where(place >= by, jnp.exp(jnp.where(place >= by, cumulative - back(cumulative, by), F32(0.0))), F32(0.0))
            for by in range(1, span_size)
        ]
        lower = [None] + [beta * dots(keys, moved_keys[by]) * within[by] for by in range(1, span_size)]
        pushed = beta * values
        weighted = beta * grown * keys
        for step in range(1, span_size):
            at_step = place == step
            push_less = jnp.zeros_like(pushed)
            weight_less = jnp.zeros_like(weighted)
            for by in range(1, step + 1):
                push_less = push_less + lower[by] * back(pushed, by)
                weight_less = weight_less + lower[by] * back(weighted, by)
            pushed = pushed - jnp.where(at_step, push_less, F32(0.0))
            weighted = weighted - jnp.where(at_step, weight_less, F32(0.0))
        left = jnp.concatenate([weighted, queries * grown], axis=0)
        sequence = lax.broadcasted_iota(jnp.int32, (2 * rows, 1), 0) % rows // span_size
        read = jnp.zeros((2 * rows, depth), F32)
        for seq in range(seq_count):
            term = jnp.dot(left, state_ref[seq, head], precision=lax.Precision.HIGHEST, preferred_element_type=F32)
            read = jnp.where(sequence == seq, term, read)
        corrections = pushed - read[:rows]
        outputs = read[rows:] + dots(queries, keys) * corrections
        for by in range(1, span_size):
            outputs = outputs + dots(queries, moved_keys[by]) * within[by] * back(corrections, by)
        scale = lax.rsqrt(dots(outputs, outputs) / depth + EPS)
        finished = (outputs * scale * out_gain * (gate * jax.nn.sigmoid(gate))).astype(BF16)
        for copy in range(out_ref.shape[0] // rows):
            out_ref[copy * rows : (copy + 1) * rows, first : first + depth] = finished


def propose(decay_rate, out_gain, terms, carried, span_size, total_heads, model_width, copies):
    def body(*refs):
        propose_body(span_size, total_heads, model_width, *refs)

    wide = carried.shape[1] * carried.shape[2]
    shape = (copies * terms[0].shape[1], wide)
    operands = [out_gain.reshape(1, -1), *terms, carried]
    (hidden,) = kernel(body, [decay_rate], operands, [(shape, BF16)])
    return hidden


def shards(
    tokens,
    norm_gain,
    w_query,
    w_key,
    w_value,
    w_gate,
    w_beta,
    w_decay,
    decay_rate,
    out_gain,
    w_out,
    state,
    prev_keys,
    prev_values,
    prev_beta,
    prev_logdecay,
    accepted,
    kv_size,
    tp_size,
):
    seq_count = state.shape[0]
    span_size = prev_keys.shape[1]
    own_rows = seq_count * span_size
    model_width, total_heads = w_beta.shape
    weights = [w_query, w_key, w_value, w_gate]
    to_next, to_previous, own_rows_wide = pack(tokens, norm_gain[None, :], weights, w_out, kv_size, own_rows)
    before = shift(to_next, kv_size, 1)
    after = shift(to_previous, kv_size, -1)
    after2 = shift(after[: to_next.shape[0]], kv_size, -1)

    beta = prev_beta.reshape(-1)
    logdecay = prev_logdecay.reshape(-1)
    carried = replay(state, prev_keys, prev_values, beta, logdecay, accepted)
    small_weights = jnp.concatenate([w_beta.T, w_decay.T], axis=0)
    packets = (to_next, before, after, after2)
    up, down, across, kept, w_out_near = project(own_rows_wide, small_weights, packets, kv_size, own_rows)
    across = shift(across, kv_size, 2 * JUMP)
    up = shift(up, kv_size, JUMP)
    down = shift(down, kv_size, -JUMP)
    ahead, behind = combine(kept, up, down, across, carried)
    ahead = shift(ahead, kv_size, 2 * JUMP)
    behind = shift(behind, kv_size, -2 * JUMP)
    terms = (kept, up, down, ahead, behind)
    members = kv_size // JUMP
    hidden = propose(decay_rate, out_gain, terms, carried, span_size, total_heads, model_width, 1)
    lower = [hidden]
    upper = [hidden]
    for step in range(members // 2):
        lower.append(shift(lower[-1], kv_size, JUMP))
        if step < members // 2 - 1:
            upper.append(shift(upper[-1], kv_size, -JUMP))
    partial = deliver([*lower[::-1], *upper[1:]], w_out_near)
    exchanged = lax.all_to_all(partial, "tp", 0, 0, tiled=True)
    finished = reduce_terms(exchanged.reshape(tp_size, own_rows, -1))
    landed = [
        piece if offset == 0 else shift(piece, kv_size, offset) for offset, piece in zip(WINDOW, finished)
    ][::-1]
    copies = spread(landed, tp_size).reshape(kv_size * own_rows, -1)
    mixed = lax.all_to_all(copies, "tp", 0, 0, tiled=True)
    mixed = settle(mixed.reshape(kv_size, own_rows, -1)).reshape(kv_size * own_rows, -1)
    return (mixed, carried)


def solution(mesh):
    in_specs = (
        P("grp", "kv"),
        P("kv"),
        P("kv", "tp"),
        P("kv", "tp"),
        P("kv", "tp"),
        P("kv", "tp"),
        P(),
        P(),
        P("tp"),
        P(),
        P("tp", "kv"),
        P(("grp", "kv"), "tp", None, None),
        P(("grp", "kv"), None, "tp", None),
        P(("grp", "kv"), None, "tp", None),
        P(("grp", "kv"), None, "tp"),
        P(("grp", "kv"), None, "tp"),
        P(("grp", "kv")),
    )
    out_specs = (P("grp", "kv"), P(("grp", "kv"), "tp", None, None))

    def per_device(*arguments):
        return shards(*arguments, kv_size=mesh.shape["kv"], tp_size=mesh.shape["tp"])

    return jax.shard_map(per_device, mesh=mesh, in_specs=in_specs, out_specs=out_specs, check_vma=False)
```

```python
import jax
import jax.numpy as jnp
from jax import lax
from jax.experimental import pallas as pl
from jax.experimental.pallas import tpu as pltpu
from jax.sharding import PartitionSpec as P


EPS = 1e-06
WINDOW = (-1, 0, 1, 2)
JUMP = len(WINDOW)
AHEAD = (0, JUMP, -JUMP, 2 * JUMP, -2 * JUMP, 3 * JUMP, -3 * JUMP, 4 * JUMP)
LANES = 128
HALF = LANES // 2
F32 = jnp.float32
BF16 = jnp.bfloat16


def near_memory(array):
    return pltpu.with_memory_space_constraint(array, pltpu.MemorySpace.VMEM)


def kernel(body, scalars, arrays, shapes, scratch=(), in_near=True, out_near=True):
    smem = pl.BlockSpec(memory_space=pltpu.SMEM)
    vmem = pl.BlockSpec(memory_space=pltpu.VMEM)
    kind = pltpu.VMEM if out_near else jax.ShapeDtypeStruct
    return pl.pallas_call(
        body,
        in_specs=[smem] * len(scalars) + [vmem] * len(arrays),
        out_specs=[vmem] * len(shapes),
        out_shape=[kind(shape, dtype) for shape, dtype in shapes],
        scratch_shapes=list(scratch),
    )(*scalars, *[near_memory(array) if in_near else array for array in arrays])


def shift(table, axis_size, by):
    return lax.ppermute(table, "kv", [(i, (i + by) % axis_size) for i in range(axis_size)])


def replay_body(beta_ref, logdecay_ref, accepted_ref, keys_ref, values_ref, state_ref, out_ref, rows_ref):
    seq_count, span_size, heads_here, depth = keys_ref.shape
    rows_ref[...] = jnp.zeros(rows_ref.shape, F32)

    def one(seq, carry):
        for position in range(span_size):
            first = position * heads_here
            keys = keys_ref[seq, position].astype(F32)
            keys = keys * lax.rsqrt(jnp.sum(keys * keys, axis=-1, keepdims=True) + EPS)
            rows_ref[first : first + heads_here, :] = keys
        key_columns = jnp.transpose(rows_ref[...])
        for head in range(heads_here):
            state = state_ref[seq, head]
            for position in range(span_size):
                row = position * heads_here + head
                spot = seq * span_size * heads_here + row
                active = accepted_ref[seq] > position
                logdecay = jnp.where(active, logdecay_ref[spot], F32(0.0))
                strength = jnp.where(active, beta_ref[spot], F32(0.0))
                column = jnp.broadcast_to(key_columns[:, row : row + 1], (depth, depth))
                state = jnp.exp(jnp.full((1, depth), logdecay, F32)) * state
                predicted = jnp.sum(column * state, axis=0, keepdims=True)
                value = values_ref[seq, position].astype(F32)[head : head + 1]
                state = state + column * (strength * (value - predicted))
            out_ref[seq, head] = state
        return carry

    lax.fori_loop(0, seq_count, one, 0)


def replay(state, prev_keys, prev_values, beta, logdecay, accepted):
    rows = -(-prev_keys.shape[1] * prev_keys.shape[2] // 8) * 8
    scratch = [pltpu.VMEM((rows, state.shape[-1]), F32)]
    scalars = [beta, logdecay, accepted]
    (carried,) = kernel(replay_body, scalars, [prev_keys, prev_values, state], [(state.shape, F32)], scratch)
    return carried


def rows_for(wide_ref, device, kv_size, own_rows):
    owners = [(device + ahead + 2 * kv_size) % kv_size for ahead in AHEAD]
    pieces = [wide_ref[pl.ds(pl.multiple_of(owner * own_rows, 8), own_rows), :] for owner in owners]
    return jnp.concatenate(pieces, axis=0)


def side_by_side(rows):
    half = rows.shape[0] // 2
    return jnp.concatenate([rows[:half], rows[half:]], axis=1).astype(BF16)


def layout(columns, own_rows):
    weights_at = 0
    gain_at = weights_at + 4 * columns
    rows_at = gain_at + 16
    return weights_at, gain_at, rows_at, len(AHEAD) * own_rows // 2


def pack_body(
    kv_size, own_rows, tokens_ref, gain_ref, wq_ref, wk_ref, wv_ref, wg_ref, next_ref, previous_ref, own_ref, wide_ref
):
    columns = gain_ref.shape[1]
    weights_at, gain_at, rows_at, half = layout(columns, own_rows)
    shard_kv = lax.axis_index("kv")
    wide_ref[...] = tokens_ref[...].astype(F32)
    own_ref[...] = rows_for(wide_ref, shard_kv, kv_size, own_rows)
    gain = jnp.concatenate([gain_ref[...]] * (wq_ref.shape[1] // columns), axis=1)
    gain = jnp.broadcast_to(gain, (16, wq_ref.shape[1]))
    for out_ref, stops in ((next_ref, (1,)), (previous_ref, (-2, -1))):
        for j, weight_ref in enumerate((wq_ref, wk_ref, wv_ref, wg_ref)):
            out_ref[weights_at + j * columns : weights_at + (j + 1) * columns, :] = weight_ref[...]
        out_ref[gain_at:rows_at, :] = gain
        for at, stop in enumerate(stops):
            rows = side_by_side(rows_for(wide_ref, shard_kv + stop, kv_size, own_rows))
            out_ref[rows_at + at * half : rows_at + (at + 1) * half, :] = rows


def pack(tokens, gain, weights, kv_size, own_rows):
    columns = tokens.shape[1]
    _, _, rows_at, half = layout(columns, own_rows)
    wide = weights[0].shape[1]

    def body(*refs):
        pack_body(kv_size, own_rows, *refs)

    shapes = [((rows_at + stops * half, wide), BF16) for stops in (1, 2)] + [((2 * half, columns), F32)]
    scratch = [pltpu.VMEM(tokens.shape, F32)]
    return kernel(body, [], [tokens, gain, *weights], shapes, scratch, in_near=False)


def split(values, wide):
    small = values[:, wide:]
    lane = lax.broadcasted_iota(jnp.int32, small.shape, 1)
    coarse = small.astype(BF16).astype(F32)
    rest = pltpu.roll(small - coarse, HALF, 1)
    return values[:, :wide].astype(BF16), jnp.where(lane < HALF, coarse, rest).astype(BF16)


def joined(terms, wide):
    small = terms[:, wide:].astype(F32)
    lane = lax.broadcasted_iota(jnp.int32, small.shape, 1)
    small = jnp.where(lane < HALF, small + pltpu.roll(small, HALF, 1), F32(0.0))
    return terms[:, :wide].astype(F32), small


def project_body(
    kv_size,
    own_rows,
    columns,
    own_rows_ref,
    small_ref,
    own_ref,
    before_ref,
    after_ref,
    after2_ref,
    up_ref,
    down_ref,
    across_ref,
    kept_ref,
    sums_ref,
):
    wide = own_ref.shape[1]
    weights_at, gain_at, rows_at, half = layout(columns, own_rows)
    shard_kv = lax.axis_index("kv")

    def taken(pay_ref, at):
        weights = [pay_ref[weights_at + j * columns : weights_at + (j + 1) * columns, :] for j in range(4)]
        gain = pay_ref[gain_at:rows_at, :columns].astype(F32)[:1]
        if at is None:
            return own_rows_ref[...], gain, weights
        both = pay_ref[rows_at + at * half : rows_at + (at + 1) * half, :].astype(F32)
        return jnp.concatenate([both[:, :columns], both[:, columns:]], axis=0), gain, weights

    parts = [taken(before_ref, 0), taken(own_ref, None), taken(after_ref, 1), taken(after2_ref, 0)]
    sums = [None] * 4
    small = None
    squares = None
    for at, (widened, gain, weights) in enumerate(parts):
        term = jnp.sum(widened * widened, axis=1, keepdims=True)
        squares = term if squares is None else squares + term
        scaled = (widened * gain).astype(BF16)
        for j in range(4):
            term = jnp.dot(scaled, weights[j], preferred_element_type=F32)
            sums[j] = term if sums[j] is None else sums[j] + term
        small_at = pl.multiple_of((shard_kv + WINDOW[at] + kv_size) % kv_size * columns, columns)
        term = lax.dot_general(
            scaled, small_ref[:, pl.ds(small_at, columns)], (((1,), (1,)), ((), ())), preferred_element_type=F32
        )
        small = term if small is None else small + term
    for j in range(4):
        sums_ref[:, j * wide : (j + 1) * wide] = sums[j]
    lane = lax.broadcasted_iota(jnp.int32, (small.shape[0], LANES), 1)
    sums_ref[:, 4 * wide :] = jnp.where(lane == HALF - 1, squares, F32(0.0))
    sums_ref[:, 4 * wide : 4 * wide + small.shape[1]] = small

    def block(ahead):
        start = AHEAD.index(ahead) * own_rows
        return sums_ref[start : start + own_rows, :]

    for out_ref, at, ahead in (
        (up_ref, 0, JUMP),
        (up_ref, 1, 3 * JUMP),
        (down_ref, 0, -JUMP),
        (down_ref, 1, -3 * JUMP),
        (across_ref, 0, 4 * JUMP),
    ):
        big, little = split(block(ahead), 4 * wide)
        out_ref[at, :, : 4 * wide] = big
        out_ref[at, :, 4 * wide :] = little
    for at, ahead in enumerate((0, 2 * JUMP, -2 * JUMP)):
        kept_ref[at] = block(ahead)


def project(own_rows_wide, small_weights, packets, kv_size, own_rows):
    columns = own_rows_wide.shape[1]
    across = 4 * packets[0].shape[1] + LANES
    shapes = [((count, own_rows, across), BF16) for count in (2, 2, 1)] + [((3, own_rows, across), F32)]

    def body(*refs):
        project_body(kv_size, own_rows, columns, *refs)

    scratch = [pltpu.VMEM((len(AHEAD) * own_rows, across), F32)]
    return kernel(body, [], [own_rows_wide, small_weights, *packets], shapes, scratch)


def combine_body(wide, kept_ref, up_ref, down_ref, across_ref, carried_ref, ahead_ref, behind_ref):
    del carried_ref
    for at, pieces, out_ref in ((1, (up_ref[1], across_ref[0]), ahead_ref), (2, (down_ref[1],), behind_ref)):
        big = kept_ref[at][:, :wide]
        small = kept_ref[at][:, wide:]
        for piece in pieces:
            more_big, more_small = joined(piece, wide)
            big = big + more_big
            small = small + more_small
        big, little = split(jnp.concatenate([big, small], axis=1), wide)
        out_ref[:, :wide] = big
        out_ref[:, wide:] = little


def combine(kept, up, down, across, carried):
    wide = kept.shape[2] - LANES

    def body(*refs):
        combine_body(wide, *refs)

    shapes = [(kept.shape[1:], BF16)] * 2
    return kernel(body, [], [kept, up, down, across, carried], shapes)


def deliver_body(rows_ref, weight_ref, out_ref):
    out_ref[...] = jnp.dot(rows_ref[...], weight_ref[...], preferred_element_type=F32).astype(BF16)


def deliver(rows, weight):
    (partial,) = kernel(deliver_body, [], [rows, weight], [((rows.shape[0], weight.shape[1]), BF16)])
    return partial


def reduce_all_body(terms_ref, out_ref):
    total = terms_ref[0].astype(F32)
    for member in range(1, terms_ref.shape[0]):
        total = total + terms_ref[member].astype(F32)
    for member in range(terms_ref.shape[0]):
        out_ref[member] = total.astype(BF16)


def reduce_all(terms):
    (copies,) = kernel(reduce_all_body, [], [terms], [(terms.shape, BF16)])
    return copies


def propose_body(
    span_size, total_heads, model_width, rate_ref, gain_ref, kept_ref, up_ref, down_ref, ahead_ref, behind_ref, state_ref, out_ref
):
    rows = kept_ref.shape[1]
    seq_count, heads_here, depth = state_ref.shape[0], state_ref.shape[1], state_ref.shape[2]
    wide = heads_here * depth

    def total(at, size):
        summed = kept_ref[0, :, at : at + size]
        for piece in (up_ref[0], down_ref[0], ahead_ref[...], behind_ref[...]):
            summed = summed + piece[:, at : at + size].astype(F32)
        return summed

    small = total(4 * wide, LANES)
    small = small + pltpu.roll(small, HALF, 1)
    lane = lax.broadcasted_iota(jnp.int32, small.shape, 1)

    def column(at):
        return jnp.sum(jnp.where(lane == at, small, F32(0.0)), axis=1, keepdims=True)

    inverse = lax.rsqrt(column(HALF - 1) / model_width + EPS)
    row = lax.broadcasted_iota(jnp.int32, (rows, 1), 0)
    place = row % span_size
    out_gain = gain_ref[...].astype(F32)

    def back(values, by):
        moved = pltpu.roll(values, by, 0)
        return jnp.where(place >= by, moved, F32(0.0))

    def dots(left, right):
        return jnp.sum(left * right, axis=1, keepdims=True)

    def unit(vectors):
        return vectors * lax.rsqrt(dots(vectors, vectors) + EPS)

    def over_lanes(values):
        return jnp.broadcast_to(values, (rows, depth))

    for head in range(heads_here):
        first = head * depth
        queries = unit(total(first, depth) * inverse) * F32(depth ** (-0.5))
        keys = unit(total(wide + first, depth) * inverse)
        values = total(2 * wide + first, depth) * inverse
        gate = total(3 * wide + first, depth) * inverse
        head_at = lax.axis_index("tp") * heads_here + head
        beta = over_lanes(jax.nn.sigmoid(column(head_at) * inverse))
        logit = over_lanes(column(total_heads + head_at) * inverse)
        softplus = jnp.maximum(logit, F32(0.0)) + jnp.log1p(jnp.exp(-jnp.abs(logit)))
        log_decay = -rate_ref[head] * softplus
        cumulative = log_decay
        for by in range(1, span_size):
            cumulative = cumulative + back(log_decay, by)
        grown = jnp.exp(cumulative)
        moved_keys = [keys] + [back(keys, by) for by in range(1, span_size)]
        within = [None] + [
            jnp.where(place >= by, jnp.exp(jnp.where(place >= by, cumulative - back(cumulative, by), F32(0.0))), F32(0.0))
            for by in range(1, span_size)
        ]
        lower = [None] + [beta * dots(keys, moved_keys[by]) * within[by] for by in range(1, span_size)]
        pushed = beta * values
        weighted = beta * grown * keys
        for step in range(1, span_size):
            at_step = place == step
            push_less = jnp.zeros_like(pushed)
            weight_less = jnp.zeros_like(weighted)
            for by in range(1, step + 1):
                push_less = push_less + lower[by] * back(pushed, by)
                weight_less = weight_less + lower[by] * back(weighted, by)
            pushed = pushed - jnp.where(at_step, push_less, F32(0.0))
            weighted = weighted - jnp.where(at_step, weight_less, F32(0.0))
        left = jnp.concatenate([weighted, queries * grown], axis=0)
        sequence = lax.broadcasted_iota(jnp.int32, (2 * rows, 1), 0) % rows // span_size
        read = jnp.zeros((2 * rows, depth), F32)
        for seq in range(seq_count):
            term = jnp.dot(left, state_ref[seq, head], precision=lax.Precision.HIGHEST, preferred_element_type=F32)
            read = jnp.where(sequence == seq, term, read)
        corrections = pushed - read[:rows]
        outputs = read[rows:] + dots(queries, keys) * corrections
        for by in range(1, span_size):
            outputs = outputs + dots(queries, moved_keys[by]) * within[by] * back(corrections, by)
        scale = lax.rsqrt(dots(outputs, outputs) / depth + EPS)
        finished = (outputs * scale * out_gain * (gate * jax.nn.sigmoid(gate))).astype(BF16)
        out_ref[:, first : first + depth] = finished


def propose(decay_rate, out_gain, terms, carried, span_size, total_heads, model_width):
    def body(*refs):
        propose_body(span_size, total_heads, model_width, *refs)

    wide = carried.shape[1] * carried.shape[2]
    shape = (terms[0].shape[1], wide)
    operands = [out_gain.reshape(1, -1), *terms, carried]
    (hidden,) = kernel(body, [decay_rate], operands, [(shape, BF16)])
    return hidden


def shards(
    tokens,
    norm_gain,
    w_query,
    w_key,
    w_value,
    w_gate,
    w_beta,
    w_decay,
    decay_rate,
    out_gain,
    w_out,
    state,
    prev_keys,
    prev_values,
    prev_beta,
    prev_logdecay,
    accepted,
    kv_size,
    tp_size,
):
    seq_count = state.shape[0]
    span_size = prev_keys.shape[1]
    own_rows = seq_count * span_size
    model_width, total_heads = w_beta.shape
    weights = [w_query, w_key, w_value, w_gate]
    to_next, to_previous, own_rows_wide = pack(tokens, norm_gain[None, :], weights, kv_size, own_rows)
    before = shift(to_next, kv_size, 1)
    after = shift(to_previous, kv_size, -1)
    after2 = shift(after[: to_next.shape[0]], kv_size, -1)

    beta = prev_beta.reshape(-1)
    logdecay = prev_logdecay.reshape(-1)
    carried = replay(state, prev_keys, prev_values, beta, logdecay, accepted)
    small_weights = jnp.concatenate([w_beta.T, w_decay.T], axis=0)
    packets = (to_next, before, after, after2)
    up, down, across, kept = project(own_rows_wide, small_weights, packets, kv_size, own_rows)
    across = shift(across, kv_size, 2 * JUMP)
    up = shift(up, kv_size, JUMP)
    down = shift(down, kv_size, -JUMP)
    ahead, behind = combine(kept, up, down, across, carried)
    ahead = shift(ahead, kv_size, 2 * JUMP)
    behind = shift(behind, kv_size, -2 * JUMP)
    terms = (kept, up, down, ahead, behind)
    hidden = propose(decay_rate, out_gain, terms, carried, span_size, total_heads, model_width)
    partial = deliver(lax.all_gather(hidden, "kv", axis=0, tiled=True), w_out)
    exchanged = lax.all_to_all(partial, "tp", 0, 0, tiled=True)
    copies = reduce_all(exchanged.reshape(tp_size, -1, exchanged.shape[1]))
    mixed = lax.all_to_all(copies.reshape(exchanged.shape), "tp", 0, 0, tiled=True)
    return (mixed, carried)


def solution(mesh):
    in_specs = (
        P("grp", "kv"),
        P("kv"),
        P("kv", "tp"),
        P("kv", "tp"),
        P("kv", "tp"),
        P("kv", "tp"),
        P(),
        P(),
        P("tp"),
        P(),
        P("tp", "kv"),
        P(("grp", "kv"), "tp", None, None),
        P(("grp", "kv"), None, "tp", None),
        P(("grp", "kv"), None, "tp", None),
        P(("grp", "kv"), None, "tp"),
        P(("grp", "kv"), None, "tp"),
        P(("grp", "kv")),
    )
    out_specs = (P("grp", "kv"), P(("grp", "kv"), "tp", None, None))

    def per_device(*arguments):
        return shards(*arguments, kv_size=mesh.shape["kv"], tp_size=mesh.shape["tp"])

    return jax.shard_map(per_device, mesh=mesh, in_specs=in_specs, out_specs=out_specs, check_vma=False)
```

```python
import jax
import jax.numpy as jnp
from jax import lax
from jax.experimental import pallas as pl
from jax.experimental.pallas import tpu as pltpu
from jax.sharding import PartitionSpec as P


EPS = 1e-06
WINDOW = (-1, 0, 1, 2)
JUMP = len(WINDOW)
NEAR_OUT = 8
AHEAD = (0, JUMP, -JUMP, 2 * JUMP, -2 * JUMP, 3 * JUMP, -3 * JUMP, 4 * JUMP)
LANES = 128
HALF = LANES // 2
F32 = jnp.float32
BF16 = jnp.bfloat16


def near_memory(array):
    return pltpu.with_memory_space_constraint(array, pltpu.MemorySpace.VMEM)


def kernel(body, scalars, arrays, shapes, scratch=(), in_near=True, out_near=True):
    smem = pl.BlockSpec(memory_space=pltpu.SMEM)
    vmem = pl.BlockSpec(memory_space=pltpu.VMEM)
    placed = out_near if isinstance(out_near, tuple) else (out_near,) * len(shapes)
    kinds = [pltpu.VMEM if one else jax.ShapeDtypeStruct for one in placed]
    return pl.pallas_call(
        body,
        in_specs=[smem] * len(scalars) + [vmem] * len(arrays),
        out_specs=[vmem] * len(shapes),
        out_shape=[kind(shape, dtype) for kind, (shape, dtype) in zip(kinds, shapes)],
        scratch_shapes=list(scratch),
    )(*scalars, *[near_memory(array) if in_near else array for array in arrays])


def shift(table, axis_size, by):
    return lax.ppermute(table, "kv", [(i, (i + by) % axis_size) for i in range(axis_size)])


def replay_body(
    beta_ref, logdecay_ref, accepted_ref, keys_ref, values_ref, state_ref, near_ref, out_ref, rows_ref
):
    seq_count, span_size, heads_here, depth = keys_ref.shape
    rows_ref[...] = jnp.zeros(rows_ref.shape, F32)

    def one(seq, carry):
        for position in range(span_size):
            first = position * heads_here
            keys = keys_ref[seq, position].astype(F32)
            keys = keys * lax.rsqrt(jnp.sum(keys * keys, axis=-1, keepdims=True) + EPS)
            rows_ref[first : first + heads_here, :] = keys
        key_columns = jnp.transpose(rows_ref[...])
        for head in range(heads_here):
            state = state_ref[seq, head]
            for position in range(span_size):
                row = position * heads_here + head
                spot = seq * span_size * heads_here + row
                active = accepted_ref[seq] > position
                logdecay = jnp.where(active, logdecay_ref[spot], F32(0.0))
                strength = jnp.where(active, beta_ref[spot], F32(0.0))
                column = jnp.broadcast_to(key_columns[:, row : row + 1], (depth, depth))
                state = jnp.exp(jnp.full((1, depth), logdecay, F32)) * state
                predicted = jnp.sum(column * state, axis=0, keepdims=True)
                value = values_ref[seq, position].astype(F32)[head : head + 1]
                state = state + column * (strength * (value - predicted))
            near_ref[seq, head] = state
            out_ref[seq, head] = state
        return carry

    lax.fori_loop(0, seq_count, one, 0)


def replay(state, prev_keys, prev_values, beta, logdecay, accepted):
    rows = -(-prev_keys.shape[1] * prev_keys.shape[2] // 8) * 8
    scratch = [pltpu.VMEM((rows, state.shape[-1]), F32)]
    scalars = [beta, logdecay, accepted]
    shapes = [(state.shape, F32)] * 2
    return kernel(replay_body, scalars, [prev_keys, prev_values, state], shapes, scratch, out_near=(True, False))


def rows_for(wide_ref, device, kv_size, own_rows):
    owners = [(device + ahead + 2 * kv_size) % kv_size for ahead in AHEAD]
    pieces = [wide_ref[pl.ds(pl.multiple_of(owner * own_rows, 8), own_rows), :] for owner in owners]
    return jnp.concatenate(pieces, axis=0)


def side_by_side(rows):
    half = rows.shape[0] // 2
    return jnp.concatenate([rows[:half], rows[half:]], axis=1).astype(BF16)


def layout(columns, own_rows):
    weights_at = 0
    gain_at = weights_at + 4 * columns
    rows_at = gain_at + 16
    return weights_at, gain_at, rows_at, len(AHEAD) * own_rows // 2


def pack_body(
    kv_size, own_rows, tokens_ref, gain_ref, wq_ref, wk_ref, wv_ref, wg_ref, next_ref, previous_ref, own_ref, wide_ref
):
    columns = gain_ref.shape[1]
    weights_at, gain_at, rows_at, half = layout(columns, own_rows)
    shard_kv = lax.axis_index("kv")
    wide_ref[...] = tokens_ref[...].astype(F32)
    own_ref[...] = rows_for(wide_ref, shard_kv, kv_size, own_rows)
    gain = jnp.concatenate([gain_ref[...]] * (wq_ref.shape[1] // columns), axis=1)
    gain = jnp.broadcast_to(gain, (16, wq_ref.shape[1]))
    for out_ref, stops in ((next_ref, (1,)), (previous_ref, (-2, -1))):
        for j, weight_ref in enumerate((wq_ref, wk_ref, wv_ref, wg_ref)):
            out_ref[weights_at + j * columns : weights_at + (j + 1) * columns, :] = weight_ref[...]
        out_ref[gain_at:rows_at, :] = gain
        for at, stop in enumerate(stops):
            rows = side_by_side(rows_for(wide_ref, shard_kv + stop, kv_size, own_rows))
            out_ref[rows_at + at * half : rows_at + (at + 1) * half, :] = rows


def pack(tokens, gain, weights, kv_size, own_rows):
    columns = tokens.shape[1]
    _, _, rows_at, half = layout(columns, own_rows)
    wide = weights[0].shape[1]

    def body(*refs):
        pack_body(kv_size, own_rows, *refs)

    shapes = [((rows_at + stops * half, wide), BF16) for stops in (1, 2)] + [((2 * half, columns), F32)]
    scratch = [pltpu.VMEM(tokens.shape, F32)]
    return kernel(body, [], [tokens, gain, *weights], shapes, scratch, in_near=False)


def split(values, wide):
    small = values[:, wide:]
    lane = lax.broadcasted_iota(jnp.int32, small.shape, 1)
    coarse = small.astype(BF16).astype(F32)
    rest = pltpu.roll(small - coarse, HALF, 1)
    return values[:, :wide].astype(BF16), jnp.where(lane < HALF, coarse, rest).astype(BF16)


def joined(terms, wide):
    small = terms[:, wide:].astype(F32)
    lane = lax.broadcasted_iota(jnp.int32, small.shape, 1)
    small = jnp.where(lane < HALF, small + pltpu.roll(small, HALF, 1), F32(0.0))
    return terms[:, :wide].astype(F32), small


def project_body(
    kv_size,
    own_rows,
    columns,
    own_rows_ref,
    small_ref,
    own_ref,
    before_ref,
    after_ref,
    after2_ref,
    up_ref,
    down_ref,
    across_ref,
    kept_ref,
    sums_ref,
):
    wide = own_ref.shape[1]
    weights_at, gain_at, rows_at, half = layout(columns, own_rows)
    shard_kv = lax.axis_index("kv")

    def taken(pay_ref, at):
        weights = [pay_ref[weights_at + j * columns : weights_at + (j + 1) * columns, :] for j in range(4)]
        gain = pay_ref[gain_at:rows_at, :columns].astype(F32)[:1]
        if at is None:
            return own_rows_ref[...], gain, weights
        both = pay_ref[rows_at + at * half : rows_at + (at + 1) * half, :].astype(F32)
        return jnp.concatenate([both[:, :columns], both[:, columns:]], axis=0), gain, weights

    parts = [taken(before_ref, 0), taken(own_ref, None), taken(after_ref, 1), taken(after2_ref, 0)]
    sums = [None] * 4
    small = None
    squares = None
    for at, (widened, gain, weights) in enumerate(parts):
        term = jnp.sum(widened * widened, axis=1, keepdims=True)
        squares = term if squares is None else squares + term
        scaled = (widened * gain).astype(BF16)
        for j in range(4):
            term = jnp.dot(scaled, weights[j], preferred_element_type=F32)
            sums[j] = term if sums[j] is None else sums[j] + term
        small_at = pl.multiple_of((shard_kv + WINDOW[at] + kv_size) % kv_size * columns, columns)
        term = lax.dot_general(
            scaled, small_ref[:, pl.ds(small_at, columns)], (((1,), (1,)), ((), ())), preferred_element_type=F32
        )
        small = term if small is None else small + term
    for j in range(4):
        sums_ref[:, j * wide : (j + 1) * wide] = sums[j]
    lane = lax.broadcasted_iota(jnp.int32, (small.shape[0], LANES), 1)
    sums_ref[:, 4 * wide :] = jnp.where(lane == HALF - 1, squares, F32(0.0))
    sums_ref[:, 4 * wide : 4 * wide + small.shape[1]] = small

    def block(ahead):
        start = AHEAD.index(ahead) * own_rows
        return sums_ref[start : start + own_rows, :]

    for out_ref, at, ahead in (
        (up_ref, 0, JUMP),
        (up_ref, 1, 3 * JUMP),
        (down_ref, 0, -JUMP),
        (down_ref, 1, -3 * JUMP),
        (across_ref, 0, 4 * JUMP),
    ):
        big, little = split(block(ahead), 4 * wide)
        out_ref[at, :, : 4 * wide] = big
        out_ref[at, :, 4 * wide :] = little
    for at, ahead in enumerate((0, 2 * JUMP, -2 * JUMP)):
        kept_ref[at] = block(ahead)


def project(own_rows_wide, small_weights, packets, kv_size, own_rows):
    columns = own_rows_wide.shape[1]
    across = 4 * packets[0].shape[1] + LANES
    shapes = [((count, own_rows, across), BF16) for count in (2, 2, 1)] + [((3, own_rows, across), F32)]

    def body(*refs):
        project_body(kv_size, own_rows, columns, *refs)

    scratch = [pltpu.VMEM((len(AHEAD) * own_rows, across), F32)]
    return kernel(body, [], [own_rows_wide, small_weights, *packets], shapes, scratch)


def combine_body(wide, kept_ref, up_ref, down_ref, across_ref, carried_ref, ahead_ref, behind_ref):
    del carried_ref
    for at, pieces, out_ref in ((1, (up_ref[1], across_ref[0]), ahead_ref), (2, (down_ref[1],), behind_ref)):
        big = kept_ref[at][:, :wide]
        small = kept_ref[at][:, wide:]
        for piece in pieces:
            more_big, more_small = joined(piece, wide)
            big = big + more_big
            small = small + more_small
        big, little = split(jnp.concatenate([big, small], axis=1), wide)
        out_ref[:, :wide] = big
        out_ref[:, wide:] = little


def combine(kept, up, down, across, carried):
    wide = kept.shape[2] - LANES

    def body(*refs):
        combine_body(wide, *refs)

    shapes = [(kept.shape[1:], BF16)] * 2
    return kernel(body, [], [kept, up, down, across, carried], shapes)


def deliver_near_body(kv_size, weight_ref, left_ref, three_ref, right_ref, out_ref):
    shard_kv = lax.axis_index("kv")
    own_rows = out_ref.shape[1]
    far_members = kv_size // NEAR_OUT
    pieces = [left_ref[0], left_ref[1], left_ref[2], three_ref[0], three_ref[1], three_ref[2], right_ref[0], right_ref[1]]
    for n, piece in enumerate(pieces):
        product = jnp.dot(piece, weight_ref[...], preferred_element_type=F32)
        for j in range(far_members):
            owner = (shard_kv + n - 4 + NEAR_OUT * (j - 2) + kv_size) % kv_size
            out_ref[owner] = product[j * own_rows : (j + 1) * own_rows].astype(BF16)


def deliver_near(w_out, left, three, right, kv_size, own_rows):
    def body(*refs):
        deliver_near_body(kv_size, *refs)

    shape = (kv_size, own_rows, w_out.shape[1])
    (partial,) = kernel(body, [], [w_out, left, three, right], [(shape, BF16)])
    return partial


def reduce_all_body(terms_ref, out_ref):
    total = terms_ref[0].astype(F32)
    for member in range(1, terms_ref.shape[0]):
        total = total + terms_ref[member].astype(F32)
    for member in range(terms_ref.shape[0]):
        out_ref[member] = total.astype(BF16)


def reduce_all(terms):
    (copies,) = kernel(reduce_all_body, [], [terms], [(terms.shape, BF16)])
    return copies


def stack_body(*refs):
    out_ref = refs[-1]
    for at, ref in enumerate(refs[:-1]):
        out_ref[at] = ref[...]


def stacked(pieces):
    (out,) = kernel(stack_body, [], pieces, [((len(pieces), *pieces[0].shape), BF16)])
    return out


def propose_body(
    span_size, total_heads, model_width, rate_ref, gain_ref, kept_ref, up_ref, down_ref, ahead_ref, behind_ref, state_ref, out_ref
):
    rows = kept_ref.shape[1]
    seq_count, heads_here, depth = state_ref.shape[0], state_ref.shape[1], state_ref.shape[2]
    wide = heads_here * depth

    def total(at, size):
        summed = kept_ref[0, :, at : at + size]
        for piece in (up_ref[0], down_ref[0], ahead_ref[...], behind_ref[...]):
            summed = summed + piece[:, at : at + size].astype(F32)
        return summed

    small = total(4 * wide, LANES)
    small = small + pltpu.roll(small, HALF, 1)
    lane = lax.broadcasted_iota(jnp.int32, small.shape, 1)

    def column(at):
        return jnp.sum(jnp.where(lane == at, small, F32(0.0)), axis=1, keepdims=True)

    inverse = lax.rsqrt(column(HALF - 1) / model_width + EPS)
    row = lax.broadcasted_iota(jnp.int32, (rows, 1), 0)
    place = row % span_size
    out_gain = gain_ref[...].astype(F32)

    def back(values, by):
        moved = pltpu.roll(values, by, 0)
        return jnp.where(place >= by, moved, F32(0.0))

    def dots(left, right):
        return jnp.sum(left * right, axis=1, keepdims=True)

    def unit(vectors):
        return vectors * lax.rsqrt(dots(vectors, vectors) + EPS)

    def over_lanes(values):
        return jnp.broadcast_to(values, (rows, depth))

    for head in range(heads_here):
        first = head * depth
        queries = unit(total(first, depth) * inverse) * F32(depth ** (-0.5))
        keys = unit(total(wide + first, depth) * inverse)
        values = total(2 * wide + first, depth) * inverse
        gate = total(3 * wide + first, depth) * inverse
        head_at = lax.axis_index("tp") * heads_here + head
        beta = over_lanes(jax.nn.sigmoid(column(head_at) * inverse))
        logit = over_lanes(column(total_heads + head_at) * inverse)
        softplus = jnp.maximum(logit, F32(0.0)) + jnp.log1p(jnp.exp(-jnp.abs(logit)))
        log_decay = -rate_ref[head] * softplus
        cumulative = log_decay
        for by in range(1, span_size):
            cumulative = cumulative + back(log_decay, by)
        grown = jnp.exp(cumulative)
        moved_keys = [keys] + [back(keys, by) for by in range(1, span_size)]
        within = [None] + [
            jnp.where(place >= by, jnp.exp(jnp.where(place >= by, cumulative - back(cumulative, by), F32(0.0))), F32(0.0))
            for by in range(1, span_size)
        ]
        lower = [None] + [beta * dots(keys, moved_keys[by]) * within[by] for by in range(1, span_size)]
        pushed = beta * values
        weighted = beta * grown * keys
        for step in range(1, span_size):
            at_step = place == step
            push_less = jnp.zeros_like(pushed)
            weight_less = jnp.zeros_like(weighted)
            for by in range(1, step + 1):
                push_less = push_less + lower[by] * back(pushed, by)
                weight_less = weight_less + lower[by] * back(weighted, by)
            pushed = pushed - jnp.where(at_step, push_less, F32(0.0))
            weighted = weighted - jnp.where(at_step, weight_less, F32(0.0))
        left = jnp.concatenate([weighted, queries * grown], axis=0)
        sequence = lax.broadcasted_iota(jnp.int32, (2 * rows, 1), 0) % rows // span_size
        read = jnp.zeros((2 * rows, depth), F32)
        for seq in range(seq_count):
            term = jnp.dot(left, state_ref[seq, head], precision=lax.Precision.HIGHEST, preferred_element_type=F32)
            read = jnp.where(sequence == seq, term, read)
        corrections = pushed - read[:rows]
        outputs = read[rows:] + dots(queries, keys) * corrections
        for by in range(1, span_size):
            outputs = outputs + dots(queries, moved_keys[by]) * within[by] * back(corrections, by)
        scale = lax.rsqrt(dots(outputs, outputs) / depth + EPS)
        finished = (outputs * scale * out_gain * (gate * jax.nn.sigmoid(gate))).astype(BF16)
        out_ref[:, first : first + depth] = finished


def propose(decay_rate, out_gain, terms, carried, span_size, total_heads, model_width):
    def body(*refs):
        propose_body(span_size, total_heads, model_width, *refs)

    wide = carried.shape[1] * carried.shape[2]
    shape = (terms[0].shape[1], wide)
    operands = [out_gain.reshape(1, -1), *terms, carried]
    (hidden,) = kernel(body, [decay_rate], operands, [(shape, BF16)])
    return hidden


def shards(
    tokens,
    norm_gain,
    w_query,
    w_key,
    w_value,
    w_gate,
    w_beta,
    w_decay,
    decay_rate,
    out_gain,
    w_out,
    state,
    prev_keys,
    prev_values,
    prev_beta,
    prev_logdecay,
    accepted,
    kv_size,
    tp_size,
):
    seq_count = state.shape[0]
    span_size = prev_keys.shape[1]
    own_rows = seq_count * span_size
    model_width, total_heads = w_beta.shape
    weights = [w_query, w_key, w_value, w_gate]
    to_next, to_previous, own_rows_wide = pack(tokens, norm_gain[None, :], weights, kv_size, own_rows)
    before = shift(to_next, kv_size, 1)
    after = shift(to_previous, kv_size, -1)
    after2 = shift(after[: to_next.shape[0]], kv_size, -1)

    beta = prev_beta.reshape(-1)
    logdecay = prev_logdecay.reshape(-1)
    carried, new_state = replay(state, prev_keys, prev_values, beta, logdecay, accepted)
    small_weights = jnp.concatenate([w_beta.T, w_decay.T], axis=0)
    packets = (to_next, before, after, after2)
    up, down, across, kept = project(own_rows_wide, small_weights, packets, kv_size, own_rows)
    across = shift(across, kv_size, 2 * JUMP)
    up = shift(up, kv_size, JUMP)
    down = shift(down, kv_size, -JUMP)
    ahead, behind = combine(kept, up, down, across, carried)
    ahead = shift(ahead, kv_size, 2 * JUMP)
    behind = shift(behind, kv_size, -2 * JUMP)
    terms = (kept, up, down, ahead, behind)
    hidden = propose(decay_rate, out_gain, terms, carried, span_size, total_heads, model_width)
    below = shift(hidden, kv_size, NEAR_OUT)
    above = shift(hidden, kv_size, -NEAR_OUT)
    opposite = shift(below, kv_size, NEAR_OUT)
    block = stacked([opposite, below, hidden, above]).reshape(4 * own_rows, -1)
    left = shift(block, kv_size, 1)
    right = shift(block, kv_size, -1)
    three = stacked([left, block, right])
    near_left = shift(three, kv_size, 3)
    near_right = shift(three[:2], kv_size, -3)
    partial = deliver_near(w_out, near_left, three, near_right, kv_size, own_rows)
    partial = partial.reshape(kv_size * own_rows, -1)
    exchanged = lax.all_to_all(partial, "tp", 0, 0, tiled=True)
    copies = reduce_all(exchanged.reshape(tp_size, -1, exchanged.shape[1]))
    mixed = lax.all_to_all(copies.reshape(exchanged.shape), "tp", 0, 0, tiled=True)
    return (mixed, new_state)


def solution(mesh):
    in_specs = (
        P("grp", "kv"),
        P("kv"),
        P("kv", "tp"),
        P("kv", "tp"),
        P("kv", "tp"),
        P("kv", "tp"),
        P(),
        P(),
        P("tp"),
        P(),
        P("tp", "kv"),
        P(("grp", "kv"), "tp", None, None),
        P(("grp", "kv"), None, "tp", None),
        P(("grp", "kv"), None, "tp", None),
        P(("grp", "kv"), None, "tp"),
        P(("grp", "kv"), None, "tp"),
        P(("grp", "kv")),
    )
    out_specs = (P("grp", "kv"), P(("grp", "kv"), "tp", None, None))

    def per_device(*arguments):
        return shards(*arguments, kv_size=mesh.shape["kv"], tp_size=mesh.shape["tp"])

    return jax.shard_map(per_device, mesh=mesh, in_specs=in_specs, out_specs=out_specs, check_vma=False)
```
